512 devices in a mesh: fs: 64 (over z, y), tp: 8 (over x, core).
Axes of the slice: x: 4, y: 8, z: 8, core: 2. Of those that a mesh axis runs over, the one named last changes fastest.
Arguments:
- tokens: bfloat16 [24576, 2048], P('fs', 'tp'), may hold values from -24 to 24
- mixer_gain: float32 [2048], replicated, may hold values from 0.1 to 1.9
- pool_input: bfloat16 [2048, 1024], P('fs', 'tp'), may hold values from -0.125 to 0.125
- group_weight: bfloat16 [8, 128, 128], P('tp'), may hold values from -0.5 to 0.5
- channel_scale: float32 [1024], P('tp'), may hold values from 0.5 to 2
- pool_output: bfloat16 [1024, 2048], P('tp', 'fs'), may hold values from -0.1875 to 0.1875
- ffn_gain: float32 [2048], replicated, may hold values from 0.1 to 1.9
- gate_weight: bfloat16 [2048, 5632], P('fs', 'tp'), may hold values from -0.125 to 0.125
- up_weight: bfloat16 [2048, 5632], P('fs', 'tp'), may hold values from -0.125 to 0.125
- down_weight: bfloat16 [5632, 2048], P('tp', 'fs'), may hold values from -0.078125 to 0.078125
- final_gain: float32 [2048], P('tp'), may hold values from 0.1 to 1.9
Outputs:
- normed_out: bfloat16 [24576, 2048], P('fs', 'tp')
The draws below stay inside these ranges and needn't reach their ends.
All inputs are finite; a program needn't handle non-finite values.
Results may differ from the reference program's by a relative error of at most 0.015.
Values may be sent and summed in bfloat16 or wider, within the bound.
A program may use at most 64 MiB of HBM per device.

```python
import math
import jax
import jax.numpy as jnp
from jax import lax

D = 2048
FF = 5632
GROUPS = 8
GROUP_DIM = 128
POOL = 1024
LENGTH = 128
TOKENS = 24576
N_TP = 8


def draw_tokens(key, part):
    base_key, column_key = jax.random.split(jax.random.fold_in(key, 11), 2)
    values = jax.random.normal(base_key, (TOKENS, D), jnp.float32)
    column_scales = jnp.exp(jax.random.uniform(column_key, (8,), jnp.float32, jnp.log(0.3), jnp.log(3.0)))
    values = values * jnp.repeat(column_scales, D // 8)[None, :]
    return jnp.clip(values, -24.0, 24.0).astype(jnp.bfloat16)


def level_of(rng, extent, cuts, least, high):
    level, own = 1.0, jax.random.fold_in(rng, 6)
    for axis_at, parts in cuts:
        heights = jnp.exp(jax.random.uniform(jax.random.fold_in(own, axis_at), (parts,), jnp.float32, least / len(cuts), high / len(cuts)))
        level = level * jnp.repeat(heights, extent[axis_at] // parts).reshape([-1 if axis == axis_at else 1 for axis in range(len(extent))])
    return level


def normal_values(rng, extent, scale, reach, cuts=(), kind=jnp.bfloat16):
    level = level_of(rng, extent, cuts, -0.22, 0.18) if cuts else 1.0
    array = jax.random.normal(rng, extent, jnp.float32) * scale * level
    return jnp.minimum(jnp.maximum(array, -reach), reach).astype(kind)


def setup_inputs(seed: int = 0) -> dict:
    keys = jax.random.split(jax.random.key(seed), 12)
    tokens = draw_tokens(jax.random.fold_in(keys[11], 71), 0)
    mixer_gain = jnp.clip(1.0 + 0.18 * jax.random.normal(keys[1], (D,), jnp.float32), 0.1, 1.9)
    pool_input = normal_values(keys[2], (D, POOL), D ** -0.5, 0.125, ((0, 64), (1, 8)))
    group_weight = normal_values(keys[3], (GROUPS, GROUP_DIM, GROUP_DIM), GROUP_DIM ** -0.5, 0.5, ((0, 8),))
    channel_scale = jnp.clip(jnp.exp(math.log(2.0) - 1.3862944 * jax.random.uniform(keys[4], (POOL,), jnp.float32) ** level_of(keys[4], (POOL,), ((0, 8),), -0.2, 0.2)), 0.5, 2.0)
    pool_output = normal_values(keys[5], (POOL, D), POOL ** -0.5, 0.1875, ((0, 8), (1, 64)))
    ffn_gain = jnp.clip(1.0 + 0.18 * jax.random.normal(keys[6], (D,), jnp.float32), 0.1, 1.9)
    gate_weight = normal_values(keys[7], (D, FF), D ** -0.5, 0.125, ((0, 64), (1, 8)))
    up_weight = normal_values(keys[8], (D, FF), D ** -0.5, 0.125, ((0, 64), (1, 8)))
    down_weight = normal_values(keys[9], (FF, D), FF ** -0.5, 0.078125, ((0, 8), (1, 64)))
    final_gain = jnp.clip(1.0 + 0.18 * jax.random.normal(keys[10], (D,), jnp.float32), 0.1, 1.9)
    return dict(tokens=tokens, mixer_gain=mixer_gain, pool_input=pool_input, group_weight=group_weight, channel_scale=channel_scale, pool_output=pool_output, ffn_gain=ffn_gain, gate_weight=gate_weight, up_weight=up_weight, down_weight=down_weight, final_gain=final_gain)


EPS = 1e-06

def rms(values, gain):
    wide = values.astype(jnp.float32)
    scaled = wide * jax.lax.rsqrt(lax.optimization_barrier(jnp.mean(wide * wide, axis=-1, keepdims=True)) + EPS)
    return scaled * gain.astype(jnp.float32)

def blocked_product(left, right, blocks):
    width = left.shape[1] // blocks
    total = jnp.zeros((left.shape[0], right.shape[1]), jnp.float32)
    for block in range(blocks):
        part = jnp.dot(left[:, block * width:(block + 1) * width], right[block * width:(block + 1) * width], preferred_element_type=jnp.float32)
        total = total + part.astype(jnp.bfloat16).astype(jnp.float32)
    return total

def reference(tokens, mixer_gain, pool_input, group_weight, channel_scale, pool_output, ffn_gain, gate_weight, up_weight, down_weight, final_gain):
    count_rows = tokens.shape[0]
    first_normed = rms(tokens, mixer_gain).astype(jnp.bfloat16)
    pooled_in = jnp.dot(first_normed, pool_input, preferred_element_type=jnp.float32).astype(jnp.bfloat16)
    grid = pooled_in.astype(jnp.float32).reshape(count_rows // LENGTH, LENGTH, GROUPS, GROUP_DIM)
    prefix = jnp.cumsum(grid, axis=1)
    counts = jnp.arange(1, LENGTH + 1, dtype=jnp.float32)[None, :, None]
    pieces = []
    for group in range(GROUPS):
        window = 2 ** (1 + group % 4)
        running = prefix[:, :, group]
        lagged = jnp.pad(running, ((0, 0), (window, 0), (0, 0)))[:, :LENGTH]
        average = (running - lagged) / jnp.minimum(counts, float(window))
        pieces.append(average - grid[:, :, group])
    pooled = jnp.stack(pieces, axis=2).astype(jnp.bfloat16).reshape(count_rows, GROUPS, GROUP_DIM)
    mapped = jnp.einsum('ngc,gcd->ngd', pooled.astype(jnp.float32), group_weight.astype(jnp.float32))
    grouped = (mapped.reshape(count_rows, GROUPS * GROUP_DIM) * channel_scale).astype(jnp.bfloat16)
    mixer_out = blocked_product(grouped, pool_output, N_TP)
    middle = (tokens.astype(jnp.float32) + mixer_out).astype(jnp.bfloat16)
    second_normed = rms(middle, ffn_gain).astype(jnp.bfloat16)
    gate = jnp.dot(second_normed, gate_weight, preferred_element_type=jnp.float32)
    upward = jnp.dot(second_normed, up_weight, preferred_element_type=jnp.float32)
    hidden = (jax.nn.silu(gate) * upward).astype(jnp.bfloat16)
    ffn_out = blocked_product(hidden, down_weight, N_TP)
    closing = middle.astype(jnp.float32) + ffn_out
    return rms(closing, final_gain).astype(jnp.bfloat16)
```

```python
import jax
import jax.numpy as jnp
from jax import lax
from jax.experimental import pallas as pl
from jax.experimental.pallas import tpu as pltpu
from jax.sharding import Mesh
from jax.sharding import PartitionSpec as P

MESH = pl.DeviceIdType.MESH
F32 = jnp.float32
BF16 = jnp.bfloat16
D = 2048
ROWS = 384
COLS = 256
LENGTH = 128
HID = 768
FS = ("z", "y")
TP = ("x", "c")
EPS = 1e-06
COPIES = 330

STREAMS = (("P", 8192), ("G0", 16384), ("G1", 16384), ("G2", 12288), ("D0", 12288), ("D1", 12288))
RATE = 46.6e3
DELAY = 2.2
WINDOW = 3


def hops(stream, sign):
    return 4 if (stream % 2 == 0) == (sign > 0) else 3


def weight_events():
    events, free = [], 0.0
    arrived, pending = {}, []
    for s in range(len(STREAMS)):
        pending.append((0.0, s, 1, 1))
    done = {}
    gate = {s: 0.0 for s in range(len(STREAMS))}
    while pending:
        pending.sort(key=lambda e: (max(e[0], free), e[1], e[2], e[3]))
        ready, s, phase, k = pending.pop(0)
        size = STREAMS[s][1] * (1 if phase == 1 else 8)
        begin = max(free, ready)
        events.append((ready, s, phase, k))
        free = begin + size / RATE
        arrive = free + DELAY
        arrived[(s, phase, k)] = arrive
        if k < 4:
            pending.append((arrive, s, phase, k + 1))
        elif phase == 1:
            earlier = done.get(s - WINDOW, 0.0)
            pending.append((max(arrive, earlier), s, 2, 1))
        else:
            done[s] = arrive
        if phase == 2 and k == 3:
            done[s] = arrive
            for i, e in enumerate(pending):
                if e[1] == s + WINDOW and e[2:] == (2, 1):
                    pending[i] = (max(e[0], arrive),) + e[1:]
    finish = {STREAMS[s][0]: arrived[(s, 2, 4)] for s in range(len(STREAMS))}
    return events, finish


def kernel(
    tok, w, mixer_gain, group_weight, channel_scale, ffn_gain, final_gain, out,
    T, M, PIN, POUT, GU, DN0, DN1, N, HT, MT, C, SQ,
    S1, Q1, U1, RL1, F1, S2, Q2, U2, RL2, F2, S3, Q3, U3, RL3, F3,
    local_sem, send_sem, recv_sem,
):
    z, y, x, c = (lax.axis_index(n) for n in ("z", "y", "x", "c"))
    me = 2 * x + c
    DN = (DN0, DN1)
    place = {"z": z, "y": y, "x": x, "c": c}
    size = {"z": 8, "y": 8, "x": 4, "c": 2}

    def near(axis, offset):
        return lax.rem(place[axis] + (offset + size[axis]), size[axis])

    def at(axis, offset):
        return {axis: near(axis, offset)}

    local_copies = [
        (tok, T.at[me]),
        (w.at[:, 0:128], PIN.at[z, y]),
        (w.at[:, 128:256], POUT.at[z, y]),
        (w.at[:, 256:1664], GU.at[z, y]),
        (w.at[0:16, 1664:2432], DN0.at[z, y]),
        (w.at[16:32, 1664:2432], DN1.at[z, y]),
    ]
    local_copies = [pltpu.make_async_copy(a, b, local_sem.at[i]) for i, (a, b) in enumerate(local_copies)]
    for copy in local_copies:
        copy.start()

    barrier = pltpu.get_barrier_semaphore()
    friends = [at("y", 1), at("y", -1), at("z", 1), at("z", -1)]
    peers = [{"x": near("x", dx), "c": near("c", dc)} for dx in range(4) for dc in range(2) if (dx, dc) != (0, 0)]
    for friend in friends + peers:
        pl.semaphore_signal(barrier, inc=1, device_id=friend, device_id_type=MESH)
    pl.semaphore_wait(barrier, len(friends) + len(peers))
    for copy in local_copies:
        copy.wait()

    sent = []

    def send(src, dst, device):
        i = len(sent)
        copy = pltpu.make_async_remote_copy(
            src_ref=src, dst_ref=dst, send_sem=send_sem.at[i], recv_sem=recv_sem.at[i],
            device_id=device, device_id_type=MESH,
        )
        copy.start()
        sent.append(copy)
        return copy

    def part(s, route, zi, yi):
        name = STREAMS[s][0]
        if name == "P":
            ref, tail = (PIN, POUT)[route], (slice(None), slice(None))
        elif name[0] == "G":
            lanes = ((0, 512), (512, 1024), (1024, 1408))[int(name[1])]
            ref, tail = GU, (pl.ds(16 * route, 16), slice(*lanes))
        else:
            ref, tail = DN[int(name[1])], (slice(None), slice(384 * route, 384 * route + 384))
        return ref.at[(zi, yi) + tail]

    def slab(s, route, phase, origin):
        whole = slice(None)
        if phase == 1:
            return part(s, route, z, origin) if route == 0 else part(s, route, origin, y)
        return part(s, route, origin, whole) if route == 0 else part(s, route, whole, origin)

    flights = {}

    def settle(s, phase, k):
        for route in range(2):
            for sign in (1, -1):
                copy = flights.pop((s, phase, k, route, sign), None)
                if copy is not None:
                    copy.wait_recv()

    def step(s, phase, k):
        if k == 1 and phase == 2:
            settle(s, 1, 3)
            settle(s, 1, 4)
        for route in range(2):
            axis = "y" if (route == 0) == (phase == 1) else "z"
            for sign in (1, -1):
                if k > 1:
                    copy = flights.get((s, phase, k - 1, route, sign))
                    if copy is not None and k <= hops(s, sign):
                        copy.wait_recv()
                        del flights[(s, phase, k - 1, route, sign)]
                if k <= hops(s, sign):
                    ref = slab(s, route, phase, near(axis, -sign * (k - 1)))
                    flights[(s, phase, k, route, sign)] = send(ref, ref, at(axis, sign))

    def finish(s):
        settle(s, 2, 3)
        settle(s, 2, 4)

    def gather(B):
        state = {}
        lo, hi = slice(0, ROWS // 2), slice(ROWS // 2, ROWS)
        right, left, other = at("x", 1), at("x", -1), at("c", 1)
        from_left, from_right, across = (2 * near("x", o) + c for o in (-1, 1, 2))

        def start():
            for half in (lo, hi):
                state["r", half] = send(B.at[me, half], B.at[me, half], right)
                mirror = hi if half is lo else lo
                state["l", mirror] = send(B.at[me, mirror], B.at[me, mirror], left)
            state["own"] = send(B.at[me], B.at[me], other)

        def over(block, half):
            ref = B.at[block, half]
            state["d", len(state)] = send(ref, ref, other)

        def relay():
            state["r", lo].wait_recv()
            ref = B.at[from_left, lo]
            state["rr"] = send(ref, ref, right)
            over(from_left, lo)
            state["l", hi].wait_recv()
            ref = B.at[from_right, hi]
            state["rl"] = send(ref, ref, left)
            over(from_right, hi)

        def rest():
            state["r", hi].wait_recv()
            over(from_left, hi)
            state["l", lo].wait_recv()
            over(from_right, lo)

        def far():
            state["rr"].wait_recv()
            over(across, lo)
            state["rl"].wait_recv()
            over(across, hi)

        def end():
            state["own"].wait_recv()
            for key, copy in state.items():
                if key[0] == "d":
                    copy.wait_recv()

        return start, relay, rest, far, end

    def scatter(S, Q, U, RL, F):
        state = {}
        n = S.shape[2]
        lo, hi = slice(0, n // 2), slice(n // 2, n)
        right, left, other = at("x", 1), at("x", -1), at("c", 1)

        def hand_over(offset):
            b = near("x", offset)
            state["q", offset] = send(S.at[b, near("c", 1)], Q.at[b], other)

        def pair(offset, half):
            b = near("x", offset)
            return S[b, c, half, :].astype(F32) + Q[b, half, :].astype(F32)

        def first():
            state["q", 2].wait_recv()
            U[2, lo, :] = pair(2, lo).astype(BF16)
            state["rr"] = send(U.at[2, lo], RL.at[lo], right)
            U[2, hi, :] = pair(2, hi).astype(BF16)
            state["rl"] = send(U.at[2, hi], RL.at[hi], left)

        def second():
            state["q", 1].wait_recv()
            U[0, hi, :] = pair(1, hi).astype(BF16)
            state["r1"] = send(U.at[0, hi], F.at[0, hi], right)
            state["q", -1].wait_recv()
            U[1, lo, :] = pair(-1, lo).astype(BF16)
            state["l0"] = send(U.at[1, lo], F.at[1, lo], left)

        def third():
            state["rr"].wait_recv()
            U[0, lo, :] = (pair(1, lo) + RL[lo, :].astype(F32)).astype(BF16)
            state["r0"] = send(U.at[0, lo], F.at[0, lo], right)
            state["rl"].wait_recv()
            U[1, hi, :] = (pair(-1, hi) + RL[hi, :].astype(F32)).astype(BF16)
            state["l1"] = send(U.at[1, hi], F.at[1, hi], left)

        def total():
            state["q", 0].wait_recv()
            for key in ("r1", "l0", "r0", "l1"):
                state[key].wait_recv()
            return pair(0, slice(0, n)) + F[0].astype(F32) + F[1].astype(F32)

        return hand_over, first, second, third, total

    def norm(B, gain):
        def rows_of(i, carry):
            rows = pl.ds(pl.multiple_of(i * 128, 128), 128)
            squares = jnp.zeros((128, COLS), F32)
            for j in range(8):
                v = B[j, rows, :].astype(F32)
                squares = squares + v * v
            r = lax.rsqrt(jnp.sum(squares, axis=1, keepdims=True) * (1.0 / D) + EPS)
            for j in range(8):
                lanes = slice(COLS * j, COLS * j + COLS)
                N[rows, lanes] = (B[j, rows, :].astype(F32) * r * gain[:, lanes]).astype(BF16)
            return carry

        lax.fori_loop(0, 3, rows_of, 0)

    gather1, gather2 = gather(T), gather(M)
    scatter1 = scatter(S1, Q1, U1, RL1, F1)
    scatters = (scatter(S2, Q2, U2, RL2, F2), scatter(S3, Q3, U3, RL3, F3))

    def mixer():
        finish(0)
        pooled_in = jnp.dot(N[...], PIN[...].reshape(D, 128), preferred_element_type=F32).astype(BF16)
        window = jnp.left_shift(jnp.int32(2), lax.rem(me, 4))
        later = lax.broadcasted_iota(jnp.int32, (LENGTH, LENGTH), 0)
        earlier = lax.broadcasted_iota(jnp.int32, (LENGTH, LENGTH), 1)
        inside = (earlier <= later) & (earlier > later - window)
        band = jnp.where(inside, 1.0, 0.0).astype(BF16)
        divisor = jnp.minimum(later + 1, window).astype(F32)
        grouped = []
        for s in range(ROWS // LENGTH):
            own = pooled_in[s * LENGTH : (s + 1) * LENGTH]
            sums = jnp.dot(band, own, preferred_element_type=F32)
            pooled = (sums / divisor - own.astype(F32)).astype(BF16)
            mapped = jnp.dot(pooled, group_weight[...], preferred_element_type=F32)
            grouped.append((mapped * channel_scale[...]).astype(BF16))
        grouped = jnp.concatenate(grouped, axis=0)
        for offset in (2, 1, -1, 0):
            b = near("x", offset)
            for core in (near("c", 1), c):
                piece = POUT[2 * b + core].reshape(COLS, 128)
                terms = lax.dot_general(grouped, piece, (((1,), (1,)), ((), ())), preferred_element_type=F32)
                S1[b, core] = terms.astype(BF16)
            scatter1[0](offset)

    def middle():
        value = (T[me].astype(F32) + scatter1[4]()).astype(BF16)
        M[me] = value
        gather2[0]()
        MT[...] = jnp.transpose(value.astype(F32))

    def silu_up(g, u):
        return g / (1.0 + jnp.exp(-g)) * u

    def hidden(first, last):
        def tile(i, carry):
            lanes = pl.ds(pl.multiple_of(i * 256, 256), 256)
            piece = GU[:, :, :, lanes].reshape(D, 256)
            acc = jnp.dot(N[...], piece, preferred_element_type=F32)
            h = silu_up(acc[:, :128], acc[:, 128:])
            HT[pl.ds(pl.multiple_of(i * 128, 128), 128), :] = jnp.transpose(h).astype(BF16)
            return carry

        lax.fori_loop(first, last, tile, 0)

    def hidden_tail():
        acc = jnp.dot(N[...], GU[:, :, :, 1280:1408].reshape(D, 128), preferred_element_type=F32)
        h = silu_up(acc, pltpu.roll(acc, 64, 1))
        lane = lax.broadcasted_iota(jnp.int32, h.shape, 1)
        HT[640:768, :] = jnp.transpose(jnp.where(lane < 64, h, 0.0)).astype(BF16)

    def down(h, S):
        finish(4 + h)
        for offset in (2, 1, -1, 0):
            b = near("x", offset)
            piece = DN[h][pl.ds(2 * b, 2)].reshape(256, HID)
            terms = jnp.dot(piece, HT[...], preferred_element_type=F32).astype(BF16)
            S[b] = terms.reshape(2, 128, ROWS)
            scatters[h][0](offset)

    def collect(h):
        C[:, h] = scatters[h][4]().reshape(8, 16, ROWS)

    def last():
        C[...] = C[...] + MT[...].reshape(8, 2, 16, ROWS)
        closing = C[...].reshape(COLS, ROWS)
        own = jnp.sum(closing * closing, axis=0, keepdims=True)
        SQ[me] = jnp.broadcast_to(own, (8, ROWS))
        copies = [send(SQ.at[me], SQ.at[me], peer) for peer in peers]
        for copy in copies:
            copy.wait_recv()
        squares = jnp.sum(SQ[...], axis=0)[0:1]
        scaled = C[...].reshape(COLS, ROWS) * lax.rsqrt(squares * (1.0 / D) + EPS)
        out[...] = (jnp.transpose(scaled) * final_gain[...]).astype(BF16)

    weights, ready = weight_events()
    plan = [(t, lambda e=e: step(*e)) for t, *e in weights]
    for fn, t in zip(gather1, (-1.0, 4.2, 6.3, 8.4, 9.6)):
        plan.append((t, fn))
    plan.append((9.7, lambda: norm(T, mixer_gain)))
    t = max(ready["P"], 11.5)
    plan.append((t, mixer))
    for fn, d in zip(scatter1[1:4], (3.5, 3.7, 7.5)):
        plan.append((t + d, fn))
    t = t + 11.7
    plan.append((t, middle))
    for fn, d in zip(gather2[1:], (4.5, 6.6, 8.7, 9.9)):
        plan.append((t + d, fn))
    plan.append((t + 10.0, lambda: norm(M, ffn_gain)))
    t = max(t + 12.0, ready["G0"], ready["G1"], ready["G2"])
    for s, d in ((1, 0), (2, 0), (3, 0)):
        plan.append((t, lambda s=s: finish(s)))
    for i, (a, b) in enumerate(((0, 2), (2, 4), (4, 5))):
        plan.append((t + 2.0 * i, lambda a=a, b=b: hidden(a, b)))
    plan.append((t + 5.0, hidden_tail))
    t = max(t + 6.0, ready["D0"])
    plan.append((t, lambda: down(0, S2)))
    for fn, d in zip(scatters[0][1:4], (2.5, 2.7, 5.0)):
        plan.append((t + d, fn))
    t = max(t + 2.0, ready["D1"])
    plan.append((t, lambda: down(1, S3)))
    for fn, d in zip(scatters[1][1:4], (2.5, 2.7, 5.0)):
        plan.append((t + d, fn))
    plan.append((t + 6.0, lambda: collect(0)))
    plan.append((t + 7.0, lambda: collect(1)))
    plan.append((t + 8.0, last))
    plan.sort(key=lambda e: e[0])
    for _, fn in plan:
        fn()
    for copy in sent:
        copy.wait_send()


def scatter_scratch(n, lanes):
    return [
        pltpu.VMEM((4, 2, n, lanes), BF16),
        pltpu.VMEM((4, n, lanes), BF16),
        pltpu.VMEM((3, n, lanes), BF16),
        pltpu.VMEM((n, lanes), BF16),
        pltpu.VMEM((2, n, lanes), BF16),
    ]


def local(
    tokens, mixer_gain, pool_input, group_weight, channel_scale, pool_output,
    ffn_gain, gate_weight, up_weight, down_weight, final_gain,
):
    main = jnp.stack([gate_weight[:, :640].reshape(32, 5, 128), up_weight[:, :640].reshape(32, 5, 128)], axis=2)
    pad = jnp.zeros((32, 64), BF16)
    w = jnp.concatenate(
        [pool_input, pool_output.T, main.reshape(32, 1280), gate_weight[:, 640:], up_weight[:, 640:], down_weight.T, pad],
        axis=1,
    )
    vmem = pl.BlockSpec(memory_space=pltpu.VMEM)
    hbm = pl.BlockSpec(memory_space=pltpu.HBM)
    return pl.pallas_call(
        kernel,
        out_shape=jax.ShapeDtypeStruct((ROWS, COLS), BF16),
        in_specs=[hbm, hbm] + [vmem] * 5,
        out_specs=vmem,
        scratch_shapes=[
            pltpu.VMEM((8, ROWS, COLS), BF16),
            pltpu.VMEM((8, ROWS, COLS), BF16),
            pltpu.VMEM((8, 8, 32, 128), BF16),
            pltpu.VMEM((8, 8, 32, 128), BF16),
            pltpu.VMEM((8, 8, 32, 1408), BF16),
            pltpu.VMEM((8, 8, 16, HID), BF16),
            pltpu.VMEM((8, 8, 16, HID), BF16),
            pltpu.VMEM((ROWS, D), BF16),
            pltpu.VMEM((HID, ROWS), BF16),
            pltpu.VMEM((COLS, ROWS), F32),
            pltpu.VMEM((8, 2, 16, ROWS), F32),
            pltpu.VMEM((8, 8, ROWS), F32),
            *scatter_scratch(ROWS, COLS),
            *scatter_scratch(128, ROWS),
            *scatter_scratch(128, ROWS),
            pltpu.SemaphoreType.DMA((6,)),
            pltpu.SemaphoreType.DMA((COPIES,)),
            pltpu.SemaphoreType.DMA((COPIES,)),
        ],
        compiler_params=pltpu.CompilerParams(
            collective_id=0, has_side_effects=True, vmem_limit_bytes=48 * 1024 * 1024
        ),
        name="layer",
    )(
        tokens, w, mixer_gain.reshape(1, D), group_weight.reshape(128, 128), channel_scale.reshape(1, 128),
        ffn_gain.reshape(1, D), final_gain.reshape(1, COLS),
    )


def solution(mesh):
    torus = Mesh(mesh.devices.reshape(8, 8, 4, 2), ("z", "y", "x", "c"))
    in_specs = (
        P(FS, TP),
        P(),
        P(FS, TP),
        P(TP, None, None),
        P(TP),
        P(TP, FS),
        P(),
        P(FS, TP),
        P(FS, TP),
        P(TP, FS),
        P(TP),
    )
    return jax.shard_map(local, mesh=torus, in_specs=in_specs, out_specs=P(FS, TP), check_vma=False)
```

```python
import jax
import jax.numpy as jnp
from jax import lax
from jax.experimental import pallas as pl
from jax.experimental.pallas import tpu as pltpu
from jax.sharding import Mesh
from jax.sharding import PartitionSpec as P

MESH = pl.DeviceIdType.MESH
F32 = jnp.float32
BF16 = jnp.bfloat16
D = 2048
ROWS = 384
COLS = 256
LENGTH = 128
HID = 768
FS = ("z", "y")
TP = ("x", "c")
EPS = 1e-06
SENDING = 96
ARRIVALS = 79

STREAMS = (
    ("PI", 0, 128, 16), ("PO", 0, 128, 16), ("G", 0, 384, 16), ("G", 384, 384, 16), ("G", 768, 384, 16),
    ("G", 1152, 256, 16), ("D0", 0, 384, 16), ("D1", 0, 384, 16),
)
DIRECT = (0, 1, 2)
LINK = {"w": (44e3, 2.9), "x": (44e3, 2.9), "d": (500e3, 1.5)}
WINDOW = 3
MIX, GATES, DOWN = (0, 1), (2, 3, 4, 5), (6, 7)


def hops(stream, sign):
    return 4 if (stream % 2 == 0) == (sign > 0) else 3


def events():
    plan = []

    def add(name, rank, needs=(), after=(), cost=0.1, sends=()):
        plan.append((name, rank, tuple(needs), tuple(after), cost, tuple(sends)))

    for s, (_, first, lanes, rows) in enumerate(STREAMS):
        piece = 2 * rows * lanes
        if s in DIRECT:
            add(("w", s, 0, 4), s - 20, sends=[(("w", s, 1, 4), "w", 8 * piece)])
        for phase in (1, 2):
            for k in range(1, 5):
                if phase == 1 and s in DIRECT:
                    continue
                needs = [("w", s, phase, k - 1)] if k > 1 else [("w", s, 1, 4)] if phase == 2 else []
                after = [("w", s - WINDOW, 2, 3)] if phase == 2 and k == 1 and s >= WINDOW else []
                size = piece * (8 if phase == 2 else 1)
                add(("w", s, phase, k), s - 10, needs, after, 0.05 if phase == 2 else 0.15, [(("w", s, phase, k), "w", size)])

    def add_gather(tag, rank, first):
        half, over = ROWS * COLS, lambda *keys: [((tag, "d", k), "d", ROWS * COLS) for k in keys]
        sends = [((tag, "near"), "x", half), ((tag, "next"), "x", half), ((tag, "own"), "d", 2 * half)]
        add((tag, 0), rank, [], first, 0.1, sends)
        add((tag, 1), rank, [(tag, "near")], [(tag, 0)], 0.1, [((tag, "far"), "x", half)] + over(0, 1))
        add((tag, 2), rank, [(tag, "next")], [(tag, 1)], 0.1, over(2, 3))
        add((tag, 3), rank, [(tag, "far")], [(tag, 2)], 0.1, over(4, 5))
        add((tag, 4), rank, [(tag, "own")] + [(tag, "d", k) for k in range(6)], [(tag, 3)])

    def add_scatter(tag, rank, source, block):
        half = block // 2
        add((tag, 1), rank, [(tag, "q", 2)], [source], 0.15, [((tag, "far"), "x", half)])
        add((tag, 2), rank, [(tag, "q", 1), (tag, "q", -1)], [(tag, 1)], 0.15, [((tag, "one"), "x", half)])
        add((tag, 3), rank, [(tag, "far")], [(tag, 2)], 0.15, [((tag, "two"), "x", half)])

    def whole(tag):
        return [(tag, "two"), (tag, "one"), (tag, "q", 0)]

    block1, block2 = 2 * ROWS * COLS, 2 * ROWS * 128
    add_gather("g1", -30, [])
    add("norm1", 0, [], [("g1", 4)], 0.7)
    add("mixer", 0, [("w", s, 2, 4) for s in MIX], ["norm1"], 2.0, [(("s1", "q", o), "d", block1) for o in (2, 1, -1, 0)])
    add_scatter("s1", -5, "mixer", block1)
    add_gather("g2", -5, ["middle"])
    add("middle", 0, whole("s1"), [("s1", 3)], 0.8)
    add("norm2", 0, [], [("g2", 4)], 0.7)
    for i in range(6):
        needs = [] if i else [("w", s, 2, 4) for s in GATES]
        add(("h", i), 0, needs, [("h", i - 1)] if i else ["norm2"], 1.1)
    for h in range(2):
        tag, before = f"s{2 + h}", ("h", 5)
        for offset in (2, 1, -1, 0):
            name = ("d", h, offset)
            add(name, h, [("w", DOWN[h], 2, 4)], [before], 0.4, [((tag, "q", offset), "d", block2)])
            before = name
        add_scatter(tag, h - 3, ("d", h, 2), block2)
        add(("c", h), h - 3, whole(tag), [(tag, 3)], 0.4)
    add("last", 9, [], [("c", 0), ("c", 1)], 4.0)
    return plan


def order(plan, margin=0.3):
    now, free, arrival, done, left, result = 0.0, {}, {}, set(), list(plan), []
    while left:
        best = None
        for e in left:
            name, rank, needs, after, cost, sends = e
            if any(k not in arrival for k in needs) or any(k not in done for k in after):
                continue
            key = (max([now] + [arrival[k] + margin for k in needs]), rank)
            if best is None or key < best[0]:
                best = (key, e)
        (ready, _), e = best
        name, rank, needs, after, cost, sends = e
        now = ready + cost
        done.add(name)
        for key, link, size in sends:
            rate, delay = LINK[link]
            free[link] = max(free.get(link, 0.0), now) + size / rate
            arrival[key] = free[link] + delay
        left.remove(e)
        result.append((ready, name))
    return result


def kernel(
    tok, pool_in, pool_out, gate, up, down_t, mixer_gain_in, group_weight_in, channel_scale_in, ffn_gain_in,
    final_gain_in, out,
    T, M, PIN, POUT, GU, DN0, DN1, N, HT, MT, C, SQ,
    gate_own, up_own, down_own, mixer_gain, group_weight, channel_scale, ffn_gain, final_gain,
    S1, Q1, U1, RL1, F1, S2, Q2, U2, RL2, F2, S3, Q3, U3, RL3, F3, W,
    local_sem, send_sem, recv_sem,
):
    z, y, x, c = (lax.axis_index(n) for n in ("z", "y", "x", "c"))
    me = 2 * x + c
    DN = (DN0, DN1)
    place = {"z": z, "y": y, "x": x, "c": c}
    size = {"z": 8, "y": 8, "x": 4, "c": 2}

    def near(axis, offset):
        return lax.rem(place[axis] + (offset + size[axis]), size[axis])

    def at(axis, offset):
        return {axis: near(axis, offset)}

    barrier = pltpu.get_barrier_semaphore()
    friends = [at(axis, o) for axis in ("y", "z") for o in (1, -1, 2, -2, 3, -3, 4)]
    peers = [{"x": near("x", dx), "c": near("c", dc)} for dx in range(4) for dc in range(2) if (dx, dc) != (0, 0)]
    for friend in friends + peers:
        pl.semaphore_signal(barrier, inc=1, device_id=friend, device_id_type=MESH)
    local_copies = [
        (gate, gate_own), (up, up_own), (down_t, down_own), (pool_in, PIN.at[z, y]), (pool_out, POUT.at[z, y]),
        (tok, T.at[me]), (mixer_gain_in, mixer_gain), (group_weight_in, group_weight),
        (channel_scale_in, channel_scale), (ffn_gain_in, ffn_gain), (final_gain_in, final_gain),
    ]
    local_copies = [pltpu.make_async_copy(a, b, local_sem.at[i]) for i, (a, b) in enumerate(local_copies)]
    for copy in local_copies:
        copy.start()

    for copy in local_copies:
        copy.wait()
    for i in range(5):
        GU[z, y, :, 256 * i : 256 * i + 128] = gate_own[:, 128 * i : 128 * i + 128]
        GU[z, y, :, 256 * i + 128 : 256 * i + 256] = up_own[:, 128 * i : 128 * i + 128]
    GU[z, y, :, 1280:1408] = jnp.concatenate([gate_own[:, 640:], up_own[:, 640:]], axis=1)
    padded = jnp.concatenate([down_own[:, 640:], jnp.zeros((32, 64), BF16)], axis=1)
    for h in range(2):
        DN[h][z, y, :, :640] = down_own[16 * h : 16 * h + 16, :640]
        DN[h][z, y, :, 640:] = padded[16 * h : 16 * h + 16]
    pl.semaphore_wait(barrier, len(friends) + len(peers))

    sent, groups = [], {}

    def send(src, dst, device, group):
        i = len(sent)
        if i >= SENDING:
            sent[i - SENDING].wait_send()
        slot, size = groups.setdefault(group, (len(groups), 0))
        bytes_of = dst.dtype.itemsize
        for n in dst.shape:
            bytes_of *= n
        groups[group] = (slot, size + bytes_of)
        copy = pltpu.make_async_remote_copy(
            src_ref=src, dst_ref=dst, send_sem=send_sem.at[i % SENDING], recv_sem=recv_sem.at[slot],
            device_id=device, device_id_type=MESH,
        )
        copy.start()
        sent.append(copy)

    def arrived(group):
        slot, size = groups[group]
        ref = W.at[pl.ds(0, size // 256)]
        pltpu.make_async_copy(ref, ref, recv_sem.at[slot]).wait()

    def part(s, route, zi, yi):
        name, first, lanes, rows = STREAMS[s]
        if name[0] == "D":
            ref, tail = DN[int(name[1])], (slice(None), pl.ds(384 * route, 384))
        else:
            ref = {"PI": PIN, "PO": POUT, "G": GU}[name]
            tail = (pl.ds(16 * route, 16), pl.ds(first, lanes))
        return ref.at[(zi, yi) + tail]

    def slab(s, route, phase, origin):
        whole = slice(None)
        if phase == 1:
            return part(s, route, z, origin) if route == 0 else part(s, route, origin, y)
        return part(s, route, origin, whole) if route == 0 else part(s, route, whole, origin)

    def spread(s):
        for route in range(2):
            axis = "yz"[route]
            ref = slab(s, route, 1, place[axis])
            for offset in (1, -1, 2, -2, 3, -3, 4):
                send(ref, ref, at(axis, offset), ("w", s, 1, 4))

    def step(s, phase, k):
        if k > 1:
            arrived(("w", s, phase, k - 1))
        elif phase == 2:
            arrived(("w", s, 1, 4))
        for route in range(2):
            axis = "y" if (route == 0) == (phase == 1) else "z"
            for sign in (1, -1):
                if k <= hops(s, sign):
                    ref = slab(s, route, phase, near(axis, -sign * (k - 1)))
                    send(ref, ref, at(axis, sign), ("w", s, phase, k))

    def finish(s):
        arrived(("w", s, 2, 4))

    def gather(B, tag):
        lo, hi = slice(0, ROWS // 2), slice(ROWS // 2, ROWS)
        right, left, other = at("x", 1), at("x", -1), at("c", 1)
        from_left, from_right, across = (2 * near("x", o) + c for o in (-1, 1, 2))

        def pass_on(block, half, device, group):
            ref = B.at[block, half]
            send(ref, ref, device, (tag, group))

        def start():
            pass_on(me, lo, right, "near")
            pass_on(me, hi, left, "near")
            pass_on(me, hi, right, "next")
            pass_on(me, lo, left, "next")
            send(B.at[me], B.at[me], other, (tag, "d"))

        def relay():
            arrived((tag, "near"))
            pass_on(from_left, lo, right, "far")
            pass_on(from_right, hi, left, "far")
            pass_on(from_left, lo, other, "d")
            pass_on(from_right, hi, other, "d")

        def rest():
            arrived((tag, "next"))
            pass_on(from_left, hi, other, "d")
            pass_on(from_right, lo, other, "d")

        def far():
            arrived((tag, "far"))
            pass_on(across, lo, other, "d")
            pass_on(across, hi, other, "d")

        def end():
            arrived((tag, "d"))

        return start, relay, rest, far, end

    def scatter(S, Q, U, RL, F, tag):
        n = S.shape[2]
        lo, hi = slice(0, n // 2), slice(n // 2, n)
        right, left, other = at("x", 1), at("x", -1), at("c", 1)

        def hand_over(offset):
            b = near("x", offset)
            send(S.at[b, near("c", 1)], Q.at[b], other, (tag, "q", abs(offset)))

        def pair(offset, half):
            b = near("x", offset)
            return S[b, c, half, :].astype(F32) + Q[b, half, :].astype(F32)

        def first():
            arrived((tag, "q", 2))
            U[2, lo, :] = pair(2, lo).astype(BF16)
            send(U.at[2, lo], RL.at[lo], right, (tag, "far"))
            U[2, hi, :] = pair(2, hi).astype(BF16)
            send(U.at[2, hi], RL.at[hi], left, (tag, "far"))

        def second():
            arrived((tag, "q", 1))
            U[0, hi, :] = pair(1, hi).astype(BF16)
            send(U.at[0, hi], F.at[0, hi], right, (tag, "near"))
            U[1, lo, :] = pair(-1, lo).astype(BF16)
            send(U.at[1, lo], F.at[1, lo], left, (tag, "near"))

        def third():
            arrived((tag, "far"))
            U[0, lo, :] = (pair(1, lo) + RL[lo, :].astype(F32)).astype(BF16)
            send(U.at[0, lo], F.at[0, lo], right, (tag, "near"))
            U[1, hi, :] = (pair(-1, hi) + RL[hi, :].astype(F32)).astype(BF16)
            send(U.at[1, hi], F.at[1, hi], left, (tag, "near"))

        def total():
            arrived((tag, "q", 0))
            arrived((tag, "near"))
            return pair(0, slice(0, n)) + F[0].astype(F32) + F[1].astype(F32)

        return hand_over, first, second, third, total

    def norm(B, gain):
        def rows_of(i, carry):
            rows = pl.ds(pl.multiple_of(i * 128, 128), 128)
            squares = jnp.zeros((128, COLS), F32)
            for j in range(8):
                v = B[j, rows, :].astype(F32)
                squares = squares + v * v
            r = lax.rsqrt(jnp.sum(squares, axis=1, keepdims=True) * (1.0 / D) + EPS)
            for j in range(8):
                lanes = slice(COLS * j, COLS * j + COLS)
                N[rows, lanes] = (B[j, rows, :].astype(F32) * r * gain[:, lanes]).astype(BF16)
            return carry

        lax.fori_loop(0, 3, rows_of, 0)

    gather1, gather2 = gather(T, "g1"), gather(M, "g2")
    scatter1 = scatter(S1, Q1, U1, RL1, F1, "s1")
    scatters = (scatter(S2, Q2, U2, RL2, F2, "s2"), scatter(S3, Q3, U3, RL3, F3, "s3"))

    def mixer():
        for s in MIX:
            finish(s)
        pooled_in = jnp.dot(N[...], PIN[...].reshape(D, 128), preferred_element_type=F32).astype(BF16)
        window = jnp.left_shift(jnp.int32(2), lax.rem(me, 4))
        later = lax.broadcasted_iota(jnp.int32, (LENGTH, LENGTH), 0)
        earlier = lax.broadcasted_iota(jnp.int32, (LENGTH, LENGTH), 1)
        inside = (earlier <= later) & (earlier > later - window)
        band = jnp.where(inside, 1.0, 0.0).astype(BF16)
        divisor = jnp.minimum(later + 1, window).astype(F32)
        grouped = []
        for s in range(ROWS // LENGTH):
            own = pooled_in[s * LENGTH : (s + 1) * LENGTH]
            sums = jnp.dot(band, own, preferred_element_type=F32)
            pooled = (sums / divisor - own.astype(F32)).astype(BF16)
            mapped = jnp.dot(pooled, group_weight[...], preferred_element_type=F32)
            grouped.append((mapped * channel_scale[...]).astype(BF16))
        grouped = jnp.concatenate(grouped, axis=0)
        for offset in (2, 1, -1, 0):
            b = near("x", offset)
            for core in (near("c", 1), c):
                piece = POUT[2 * b + core].reshape(COLS, 128)
                terms = lax.dot_general(grouped, piece, (((1,), (1,)), ((), ())), preferred_element_type=F32)
                S1[b, core] = terms.astype(BF16)
            scatter1[0](offset)

    def middle():
        value = (T[me].astype(F32) + scatter1[4]()).astype(BF16)
        M[me] = value
        gather2[0]()
        MT[...] = jnp.transpose(value.astype(F32))

    def silu_up(g, u):
        return g / (1.0 + jnp.exp(-g)) * u

    def hidden(i):
        if i == 0:
            for s in GATES:
                finish(s)
        piece = GU[:, :, :, 256 * i : 256 * i + 256].reshape(D, 256)
        acc = jnp.dot(N[...], piece, preferred_element_type=F32)
        h = silu_up(acc[:, :128], acc[:, 128:])
        HT[128 * i : 128 * i + 128, :] = jnp.transpose(h).astype(BF16)

    def hidden_tail():
        acc = jnp.dot(N[...], GU[:, :, :, 1280:1408].reshape(D, 128), preferred_element_type=F32)
        h = silu_up(acc, pltpu.roll(acc, 64, 1))
        lane = lax.broadcasted_iota(jnp.int32, h.shape, 1)
        HT[640:768, :] = jnp.transpose(jnp.where(lane < 64, h, 0.0)).astype(BF16)

    def down(h, S, offset):
        if offset == 2:
            finish(DOWN[h])
        b = near("x", offset)
        piece = DN[h][pl.ds(2 * b, 2)].reshape(256, HID)
        terms = jnp.dot(piece, HT[...], preferred_element_type=F32).astype(BF16)
        S[b] = terms.reshape(2, 128, ROWS)
        scatters[h][0](offset)

    def collect(h):
        C[:, h] = scatters[h][4]().reshape(8, 16, ROWS)

    def last():
        C[...] = C[...] + MT[...].reshape(8, 2, 16, ROWS)
        closing = C[...].reshape(COLS, ROWS)
        own = jnp.sum(closing * closing, axis=0, keepdims=True)
        SQ[me] = jnp.broadcast_to(own, (8, ROWS))
        for peer in peers:
            send(SQ.at[me], SQ.at[me], peer, "squares")
        arrived("squares")
        squares = jnp.sum(SQ[...], axis=0)[0:1]
        scaled = C[...].reshape(COLS, ROWS) * lax.rsqrt(squares * (1.0 / D) + EPS)
        out[...] = (jnp.transpose(scaled) * final_gain[...]).astype(BF16)

    runs = {"norm1": lambda: norm(T, mixer_gain), "mixer": mixer, "middle": middle, "norm2": lambda: norm(M, ffn_gain)}
    for s in range(len(STREAMS)):
        runs["w", s, 0, 4] = lambda s=s: spread(s)
        for phase in (1, 2):
            for k in range(1, 5):
                runs["w", s, phase, k] = lambda s=s, phase=phase, k=k: step(s, phase, k)
    for tag, parts in (("g1", gather1), ("g2", gather2), ("s1", scatter1), ("s2", scatters[0]), ("s3", scatters[1])):
        for i, part_run in enumerate(parts):
            runs[tag, i] = part_run
    runs["g2", 0] = lambda: None
    for i in range(5):
        runs["h", i] = lambda i=i: hidden(i)
    runs["h", 5] = hidden_tail
    for h, S in enumerate((S2, S3)):
        runs["c", h] = lambda h=h: collect(h)
        for offset in (2, 1, -1, 0):
            runs["d", h, offset] = lambda h=h, S=S, offset=offset: down(h, S, offset)
    runs["last"] = last
    for t, name in order(events()):
        runs[name]()
    for copy in sent[-SENDING:]:
        copy.wait_send()


def scatter_scratch(n, lanes):
    return [
        pltpu.VMEM((4, 2, n, lanes), BF16),
        pltpu.VMEM((4, n, lanes), BF16),
        pltpu.VMEM((3, n, lanes), BF16),
        pltpu.VMEM((n, lanes), BF16),
        pltpu.VMEM((2, n, lanes), BF16),
    ]


def local(
    tokens, mixer_gain, pool_input, group_weight, channel_scale, pool_output,
    ffn_gain, gate_weight, up_weight, down_weight, final_gain,
):
    vmem = pl.BlockSpec(memory_space=pltpu.VMEM)
    hbm = pl.BlockSpec(memory_space=pltpu.HBM)
    return pl.pallas_call(
        kernel,
        out_shape=jax.ShapeDtypeStruct((ROWS, COLS), BF16),
        in_specs=[hbm] * 11,
        out_specs=vmem,
        scratch_shapes=[
            pltpu.VMEM((8, ROWS, COLS), BF16),
            pltpu.VMEM((8, ROWS, COLS), BF16),
            pltpu.VMEM((8, 8, 32, 128), BF16),
            pltpu.VMEM((8, 8, 32, 128), BF16),
            pltpu.VMEM((8, 8, 32, 1408), BF16),
            pltpu.VMEM((8, 8, 16, HID), BF16),
            pltpu.VMEM((8, 8, 16, HID), BF16),
            pltpu.VMEM((ROWS, D), BF16),
            pltpu.VMEM((HID, ROWS), BF16),
            pltpu.VMEM((COLS, ROWS), F32),
            pltpu.VMEM((8, 2, 16, ROWS), F32),
            pltpu.VMEM((8, 8, ROWS), F32),
            pltpu.VMEM((32, 704), BF16),
            pltpu.VMEM((32, 704), BF16),
            pltpu.VMEM((32, 704), BF16),
            pltpu.VMEM((1, D), F32),
            pltpu.VMEM((128, 128), BF16),
            pltpu.VMEM((1, 128), F32),
            pltpu.VMEM((1, D), F32),
            pltpu.VMEM((1, COLS), F32),
            *scatter_scratch(ROWS, COLS),
            *scatter_scratch(128, ROWS),
            *scatter_scratch(128, ROWS),
            pltpu.VMEM((3072, 128), BF16),
            pltpu.SemaphoreType.DMA((11,)),
            pltpu.SemaphoreType.DMA((SENDING,)),
            pltpu.SemaphoreType.DMA((ARRIVALS,)),
        ],
        compiler_params=pltpu.CompilerParams(
            collective_id=0, has_side_effects=True, vmem_limit_bytes=67043328
        ),
        name="layer",
    )(
        tokens, pool_input, pool_output.T, gate_weight, up_weight, down_weight.T, mixer_gain.reshape(1, D), group_weight.reshape(128, 128), channel_scale.reshape(1, 128),
        ffn_gain.reshape(1, D), final_gain.reshape(1, COLS),
    )


def solution(mesh):
    torus = Mesh(mesh.devices.reshape(8, 8, 4, 2), ("z", "y", "x", "c"))
    in_specs = (
        P(FS, TP),
        P(),
        P(FS, TP),
        P(TP, None, None),
        P(TP),
        P(TP, FS),
        P(),
        P(FS, TP),
        P(FS, TP),
        P(TP, FS),
        P(TP),
    )
    return jax.shard_map(local, mesh=torus, in_specs=in_specs, out_specs=P(FS, TP), check_vma=False)
```

```python
import jax
import jax.numpy as jnp
from jax import lax
from jax.experimental import pallas as pl
from jax.experimental.pallas import tpu as pltpu
from jax.sharding import Mesh
from jax.sharding import PartitionSpec as P

MESH = pl.DeviceIdType.MESH
F32 = jnp.float32
BF16 = jnp.bfloat16
D = 2048
ROWS = 384
COLS = 256
LENGTH = 128
HID = 768
FS = ("z", "y")
TP = ("x", "c")
EPS = 1e-06
SENDING = 96
ARRIVALS = 79

STREAMS = (
    ("PI", 0, 128, 16), ("PO", 0, 128, 16), ("G", 0, 256, 16), ("G", 256, 384, 16), ("G", 640, 384, 16),
    ("G", 1024, 384, 16), ("D0", 0, 384, 16), ("D1", 0, 384, 16),
)
DIRECT = (0, 1, 2)
LINK = {1: (46.6e3, 2.9), -1: (46.6e3, 2.9), "x": (46.6e3, 2.9), "d": (500e3, 1.5)}
WINDOW = 3
MIX, GATES, DOWN = (0, 1), (2, 3, 4, 5), (6, 7)


def hops(stream, phase, sign):
    return 4 if phase == 2 or (stream % 2 == 0) == (sign > 0) else 3


def tile_streams(i):
    return [s for s in GATES if STREAMS[s][1] < 256 * i + 256 and STREAMS[s][1] + STREAMS[s][2] > 256 * i]


def events():
    plan = []

    def add(name, rank, needs=(), after=(), cost=0.1, sends=()):
        plan.append((name, rank, tuple(needs), tuple(after), cost, tuple(sends)))

    for s, (_, first, lanes, rows) in enumerate(STREAMS):
        piece = 2 * rows * lanes
        if s in DIRECT:
            add(("w", s, 0, 4), s - 20, sends=[(("w", s, 1, 4), sign, 8 * piece) for sign in (1, -1)])
        for phase in (1, 2):
            for k in range(1, 5):
                if phase == 1 and s in DIRECT:
                    continue
                needs = [("w", s, phase, k - 1)] if k > 1 else [("w", s, 1, 4)] if phase == 2 else []
                after = [("w", s - WINDOW, 2, 2)] if phase == 2 and k == 1 and s >= WINDOW else []
                size = piece * (8 if phase == 2 else 1)
                cost = 0.05 if phase == 2 else 0.15
                size = size // 2 if (phase, k) == (2, 4) else size
                sends = [(("w", s, phase, k), sign, size) for sign in (1, -1) if k <= hops(s, phase, sign)]
                add(("w", s, phase, k), s - 10, needs, after, cost, sends)

    def add_gather(tag, rank, first):
        half, over = ROWS * COLS, lambda *keys: [((tag, "d", k), "d", ROWS * COLS) for k in keys]
        sends = [((tag, "near"), "x", half), ((tag, "next"), "x", half), ((tag, "own"), "d", 2 * half)]
        add((tag, 0), rank, [], first, 0.1, sends)
        add((tag, 1), rank, [(tag, "near")], [(tag, 0)], 0.1, [((tag, "far"), "x", half)] + over(0, 1))
        add((tag, 2), rank, [(tag, "next")], [(tag, 1)], 0.1, over(2, 3))
        add((tag, 3), rank, [(tag, "far")], [(tag, 2)], 0.1, over(4, 5))
        add((tag, 4), rank, [(tag, "own")] + [(tag, "d", k) for k in range(6)], [(tag, 3)])

    def add_scatter(tag, rank, source, block):
        half = block // 2
        add((tag, 1), rank, [(tag, "q", 2)], [source], 0.15, [((tag, "far"), "x", half)])
        add((tag, 2), rank, [(tag, "q", 1), (tag, "q", -1)], [(tag, 1)], 0.15, [((tag, "one"), "x", half)])
        add((tag, 3), rank, [(tag, "far")], [(tag, 2)], 0.15, [((tag, "two"), "x", half)])

    def whole(tag):
        return [(tag, "two"), (tag, "one"), (tag, "q", 0)]

    block1, block2 = 2 * ROWS * COLS, 2 * ROWS * 128
    add_gather("g1", -30, [])
    add("norm1", 0, [], [("g1", 4)], 0.7)
    add("mixer", 0, [("w", s, 2, 4) for s in MIX], ["norm1"], 2.0, [(("s1", "q", o), "d", block1) for o in (2, 1, -1, 0)])
    add_scatter("s1", -5, "mixer", block1)
    add_gather("g2", -5, ["middle"])
    add("middle", 0, whole("s1"), [("s1", 3)], 0.8)
    add("norm2", 0, [], [("g2", 4)], 0.7)
    for i in range(6):
        add(("h", i), 0, [("w", s, 2, 4) for s in tile_streams(i)], [("h", i - 1)] if i else ["norm2"], 1.06)
    for h in range(2):
        tag, before = f"s{2 + h}", ("h", 5)
        for offset in (2, 1, -1, 0):
            name = ("d", h, offset)
            add(name, h, [("w", DOWN[h], 2, 4)], [before], 0.4, [((tag, "q", offset), "d", block2)])
            before = name
        add_scatter(tag, h - 3, ("d", h, 2), block2)
        add(("c", h), h - 3, whole(tag), [(tag, 3)], 0.4)
    add("last", 9, [], [("c", 0), ("c", 1)], 4.0)
    return plan


def order(plan, margin=0.3):
    now, free, arrival, done, left, result = 0.0, {}, {}, set(), list(plan), []
    while left:
        best = None
        for e in left:
            name, rank, needs, after, cost, sends = e
            if any(k not in arrival for k in needs) or any(k not in done for k in after):
                continue
            key = (max([now] + [arrival[k] + margin for k in needs]), rank)
            if best is None or key < best[0]:
                best = (key, e)
        (ready, _), e = best
        name, rank, needs, after, cost, sends = e
        now = ready + cost
        done.add(name)
        for key, link, size in sends:
            rate, delay = LINK[link]
            free[link] = max(free.get(link, 0.0), now) + size / rate
            arrival[key] = max(arrival.get(key, 0.0), free[link] + delay)
        left.remove(e)
        result.append((ready, name))
    return result


def kernel(
    tok, pool_in, pool_out, gate, up, down_t, mixer_gain_in, group_weight_in, channel_scale_in, ffn_gain_in, out,
    T, M, PIN, POUT, GU, DN0, DN1, N, HT, MT, C, SQ,
    gate_own, up_own, down_own, mixer_gain, group_weight, channel_scale, ffn_gain,
    S1, Q1, U1, RL1, F1, S2, Q2, U2, RL2, F2, S3, Q3, U3, RL3, F3, W,
    local_sem, send_sem, recv_sem,
):
    z, y, x, c = (lax.axis_index(n) for n in ("z", "y", "x", "c"))
    me = 2 * x + c
    DN = (DN0, DN1)
    place = {"z": z, "y": y, "x": x, "c": c}
    size = {"z": 8, "y": 8, "x": 4, "c": 2}

    def near(axis, offset):
        return lax.rem(place[axis] + (offset + size[axis]), size[axis])

    def at(axis, offset):
        return {axis: near(axis, offset)}

    barrier = pltpu.get_barrier_semaphore()
    friends = [at(axis, o) for axis in ("y", "z") for o in (1, -1, 2, -2, 3, -3, 4)]
    peers = [{"x": near("x", dx), "c": near("c", dc)} for dx in range(4) for dc in range(2) if (dx, dc) != (0, 0)]
    for friend in friends + peers:
        pl.semaphore_signal(barrier, inc=1, device_id=friend, device_id_type=MESH)
    local_copies = [
        (gate, gate_own), (up, up_own), (down_t, down_own), (pool_in, PIN.at[z, y]), (pool_out, POUT.at[z, y]),
        (tok, T.at[me]), (mixer_gain_in, mixer_gain), (group_weight_in, group_weight),
        (channel_scale_in, channel_scale), (ffn_gain_in, ffn_gain),
    ]
    local_copies = [pltpu.make_async_copy(a, b, local_sem.at[i]) for i, (a, b) in enumerate(local_copies)]
    for copy in local_copies:
        copy.start()

    for copy in local_copies:
        copy.wait()
    for i in range(5):
        GU[z, y, :, 256 * i : 256 * i + 128] = gate_own[:, 128 * i : 128 * i + 128]
        GU[z, y, :, 256 * i + 128 : 256 * i + 256] = up_own[:, 128 * i : 128 * i + 128]
    GU[z, y, :, 1280:1408] = jnp.concatenate([gate_own[:, 640:], up_own[:, 640:]], axis=1)
    padded = jnp.concatenate([down_own[:, 640:], jnp.zeros((32, 64), BF16)], axis=1)
    for h in range(2):
        DN[h][z, y, :, :640] = down_own[16 * h : 16 * h + 16, :640]
        DN[h][z, y, :, 640:] = padded[16 * h : 16 * h + 16]
    pl.semaphore_wait(barrier, len(friends) + len(peers))

    sent, groups = [], {}

    def send(src, dst, device, group):
        i = len(sent)
        if i >= SENDING:
            sent[i - SENDING].wait_send()
        slot, size = groups.setdefault(group, (len(groups), 0))
        bytes_of = dst.dtype.itemsize
        for n in dst.shape:
            bytes_of *= n
        groups[group] = (slot, size + bytes_of)
        copy = pltpu.make_async_remote_copy(
            src_ref=src, dst_ref=dst, send_sem=send_sem.at[i % SENDING], recv_sem=recv_sem.at[slot],
            device_id=device, device_id_type=MESH,
        )
        copy.start()
        sent.append(copy)

    def arrived(group):
        slot, size = groups[group]
        ref = W.at[pl.ds(0, size // 256)]
        pltpu.make_async_copy(ref, ref, recv_sem.at[slot]).wait()

    def part(s, route, zi, yi):
        name, first, lanes, rows = STREAMS[s]
        if name[0] == "D":
            ref, tail = DN[int(name[1])], (slice(None), pl.ds(384 * route, 384))
        else:
            ref = {"PI": PIN, "PO": POUT, "G": GU}[name]
            tail = (pl.ds(16 * route, 16), pl.ds(first, lanes))
        return ref.at[(zi, yi) + tail]

    def slab(s, route, phase, origin, whole=slice(None)):
        if phase == 1:
            return part(s, route, z, origin) if route == 0 else part(s, route, origin, y)
        return part(s, route, origin, whole) if route == 0 else part(s, route, whole, origin)

    def spread(s):
        for route in range(2):
            axis = "yz"[route]
            ref = slab(s, route, 1, place[axis])
            for offset in (1, -1, 2, -2, 3, -3, 4):
                send(ref, ref, at(axis, offset), ("w", s, 1, 4))

    def step(s, phase, k):
        if k > 1:
            arrived(("w", s, phase, k - 1))
        elif phase == 2:
            arrived(("w", s, 1, 4))
        for route in range(2):
            axis = "y" if (route == 0) == (phase == 1) else "z"
            for sign in (1, -1):
                if k <= hops(s, phase, sign):
                    pieces = slice(None) if (phase, k) != (2, 4) else slice(0, 4) if sign > 0 else slice(4, 8)
                    ref = slab(s, route, phase, near(axis, -sign * (k - 1)), pieces)
                    send(ref, ref, at(axis, sign), ("w", s, phase, k))

    def finish(s):
        arrived(("w", s, 2, 4))

    def gather(B, tag):
        lo, hi = slice(0, ROWS // 2), slice(ROWS // 2, ROWS)
        right, left, other = at("x", 1), at("x", -1), at("c", 1)
        from_left, from_right, across = (2 * near("x", o) + c for o in (-1, 1, 2))

        def pass_on(block, half, device, group):
            ref = B.at[block, half]
            send(ref, ref, device, (tag, group))

        def start():
            pass_on(me, lo, right, "near")
            pass_on(me, hi, left, "near")
            pass_on(me, hi, right, "next")
            pass_on(me, lo, left, "next")
            send(B.at[me], B.at[me], other, (tag, "d"))

        def relay():
            arrived((tag, "near"))
            pass_on(from_left, lo, right, "far")
            pass_on(from_right, hi, left, "far")
            pass_on(from_left, lo, other, "d")
            pass_on(from_right, hi, other, "d")

        def rest():
            arrived((tag, "next"))
            pass_on(from_left, hi, other, "d")
            pass_on(from_right, lo, other, "d")

        def far():
            arrived((tag, "far"))
            pass_on(across, lo, other, "d")
            pass_on(across, hi, other, "d")

        def end():
            arrived((tag, "d"))

        return start, relay, rest, far, end

    def scatter(S, Q, U, RL, F, tag):
        n = S.shape[2]
        lo, hi = slice(0, n // 2), slice(n // 2, n)
        right, left, other = at("x", 1), at("x", -1), at("c", 1)

        def hand_over(offset):
            b = near("x", offset)
            send(S.at[b, near("c", 1)], Q.at[b], other, (tag, "q", abs(offset)))

        def pair(offset, half):
            b = near("x", offset)
            return S[b, c, half, :].astype(F32) + Q[b, half, :].astype(F32)

        def first():
            arrived((tag, "q", 2))
            U[2, lo, :] = pair(2, lo).astype(BF16)
            send(U.at[2, lo], RL.at[lo], right, (tag, "far"))
            U[2, hi, :] = pair(2, hi).astype(BF16)
            send(U.at[2, hi], RL.at[hi], left, (tag, "far"))

        def second():
            arrived((tag, "q", 1))
            U[0, hi, :] = pair(1, hi).astype(BF16)
            send(U.at[0, hi], F.at[0, hi], right, (tag, "near"))
            U[1, lo, :] = pair(-1, lo).astype(BF16)
            send(U.at[1, lo], F.at[1, lo], left, (tag, "near"))

        def third():
            arrived((tag, "far"))
            U[0, lo, :] = (pair(1, lo) + RL[lo, :].astype(F32)).astype(BF16)
            send(U.at[0, lo], F.at[0, lo], right, (tag, "near"))
            U[1, hi, :] = (pair(-1, hi) + RL[hi, :].astype(F32)).astype(BF16)
            send(U.at[1, hi], F.at[1, hi], left, (tag, "near"))

        def total():
            arrived((tag, "q", 0))
            arrived((tag, "near"))
            return pair(0, slice(0, n)) + F[0].astype(F32) + F[1].astype(F32)

        return hand_over, first, second, third, total

    def norm(B, gain):
        def rows_of(i, carry):
            rows = pl.ds(pl.multiple_of(i * 128, 128), 128)
            squares = jnp.zeros((128, COLS), F32)
            for j in range(8):
                v = B[j, rows, :].astype(F32)
                squares = squares + v * v
            r = lax.rsqrt(jnp.sum(squares, axis=1, keepdims=True) * (1.0 / D) + EPS)
            for j in range(8):
                lanes = slice(COLS * j, COLS * j + COLS)
                N[rows, lanes] = (B[j, rows, :].astype(F32) * r * gain[:, lanes]).astype(BF16)
            return carry

        lax.fori_loop(0, 3, rows_of, 0)

    gather1, gather2 = gather(T, "g1"), gather(M, "g2")
    scatter1 = scatter(S1, Q1, U1, RL1, F1, "s1")
    scatters = (scatter(S2, Q2, U2, RL2, F2, "s2"), scatter(S3, Q3, U3, RL3, F3, "s3"))

    def mixer():
        for s in MIX:
            finish(s)
        pooled_in = jnp.dot(N[...], PIN[...].reshape(D, 128), preferred_element_type=F32).astype(BF16)
        window = jnp.left_shift(jnp.int32(2), lax.rem(me, 4))
        later = lax.broadcasted_iota(jnp.int32, (LENGTH, LENGTH), 0)
        earlier = lax.broadcasted_iota(jnp.int32, (LENGTH, LENGTH), 1)
        inside = (earlier <= later) & (earlier > later - window)
        band = jnp.where(inside, 1.0, 0.0).astype(BF16)
        divisor = jnp.minimum(later + 1, window).astype(F32)
        grouped = []
        for s in range(ROWS // LENGTH):
            own = pooled_in[s * LENGTH : (s + 1) * LENGTH]
            sums = jnp.dot(band, own, preferred_element_type=F32)
            pooled = (sums / divisor - own.astype(F32)).astype(BF16)
            mapped = jnp.dot(pooled, group_weight[...], preferred_element_type=F32)
            grouped.append((mapped * channel_scale[...]).astype(BF16))
        grouped = jnp.concatenate(grouped, axis=0)
        for offset in (2, 1, -1, 0):
            b = near("x", offset)
            for core in (near("c", 1), c):
                piece = POUT[2 * b + core].reshape(COLS, 128)
                terms = lax.dot_general(grouped, piece, (((1,), (1,)), ((), ())), preferred_element_type=F32)
                S1[b, core] = terms.astype(BF16)
            scatter1[0](offset)

    def middle():
        value = (T[me].astype(F32) + scatter1[4]()).astype(BF16)
        M[me] = value
        gather2[0]()
        MT[...] = jnp.transpose(value.astype(F32))

    def silu_up(g, u):
        return g / (1.0 + jnp.exp(-g)) * u

    settled = set()

    def settle(i):
        for s in tile_streams(i):
            if s not in settled:
                finish(s)
                settled.add(s)

    def hidden(i):
        settle(i)
        piece = GU[:, :, :, 256 * i : 256 * i + 256].reshape(D, 256)
        acc = jnp.dot(N[...], piece, preferred_element_type=F32)
        h = silu_up(acc[:, :128], acc[:, 128:])
        HT[128 * i : 128 * i + 128, :] = jnp.transpose(h).astype(BF16)

    def hidden_tail():
        settle(5)
        acc = jnp.dot(N[...], GU[:, :, :, 1280:1408].reshape(D, 128), preferred_element_type=F32)
        h = silu_up(acc, pltpu.roll(acc, 64, 1))
        lane = lax.broadcasted_iota(jnp.int32, h.shape, 1)
        HT[640:768, :] = jnp.transpose(jnp.where(lane < 64, h, 0.0)).astype(BF16)

    def down(h, S, offset):
        if offset == 2:
            finish(DOWN[h])
        b = near("x", offset)
        piece = DN[h][pl.ds(2 * b, 2)].reshape(256, HID)
        terms = jnp.dot(piece, HT[...], preferred_element_type=F32).astype(BF16)
        S[b] = terms.reshape(2, 128, ROWS)
        scatters[h][0](offset)

    def collect(h):
        C[:, h] = scatters[h][4]().reshape(8, 16, ROWS)

    def last():
        C[...] = C[...] + MT[...].reshape(8, 2, 16, ROWS)
        closing = C[...].reshape(COLS, ROWS)
        own = jnp.sum(closing * closing, axis=0, keepdims=True)
        SQ[me] = jnp.broadcast_to(own, (8, ROWS))
        for peer in peers:
            send(SQ.at[me], SQ.at[me], peer, "squares")
        arrived("squares")
        squares = jnp.sum(SQ[...], axis=0)[0:1]
        scaled = C[...].reshape(COLS, ROWS) * lax.rsqrt(squares * (1.0 / D) + EPS)
        out[...] = jnp.transpose(scaled)

    runs = {"norm1": lambda: norm(T, mixer_gain), "mixer": mixer, "middle": middle, "norm2": lambda: norm(M, ffn_gain)}
    for s in range(len(STREAMS)):
        runs["w", s, 0, 4] = lambda s=s: spread(s)
        for phase in (1, 2):
            for k in range(1, 5):
                runs["w", s, phase, k] = lambda s=s, phase=phase, k=k: step(s, phase, k)
    for tag, parts in (("g1", gather1), ("g2", gather2), ("s1", scatter1), ("s2", scatters[0]), ("s3", scatters[1])):
        for i, part_run in enumerate(parts):
            runs[tag, i] = part_run
    runs["g2", 0] = lambda: None
    for i in range(5):
        runs["h", i] = lambda i=i: hidden(i)
    runs["h", 5] = hidden_tail
    for h, S in enumerate((S2, S3)):
        runs["c", h] = lambda h=h: collect(h)
        for offset in (2, 1, -1, 0):
            runs["d", h, offset] = lambda h=h, S=S, offset=offset: down(h, S, offset)
    runs["last"] = last
    for t, name in order(events()):
        runs[name]()
    for copy in sent[-SENDING:]:
        copy.wait_send()


def scatter_scratch(n, lanes):
    return [
        pltpu.VMEM((4, 2, n, lanes), BF16),
        pltpu.VMEM((4, n, lanes), BF16),
        pltpu.VMEM((3, n, lanes), BF16),
        pltpu.VMEM((n, lanes), BF16),
        pltpu.VMEM((2, n, lanes), BF16),
    ]


def local(
    tokens, mixer_gain, pool_input, group_weight, channel_scale, pool_output,
    ffn_gain, gate_weight, up_weight, down_weight, final_gain,
):
    vmem = pl.BlockSpec(memory_space=pltpu.VMEM)
    hbm = pl.BlockSpec(memory_space=pltpu.HBM)
    scaled = pl.pallas_call(
        kernel,
        out_shape=jax.ShapeDtypeStruct((ROWS, COLS), F32),
        in_specs=[hbm] * 10,
        out_specs=vmem,
        scratch_shapes=[
            pltpu.VMEM((8, ROWS, COLS), BF16),
            pltpu.VMEM((8, ROWS, COLS), BF16),
            pltpu.VMEM((8, 8, 32, 128), BF16),
            pltpu.VMEM((8, 8, 32, 128), BF16),
            pltpu.VMEM((8, 8, 32, 1408), BF16),
            pltpu.VMEM((8, 8, 16, HID), BF16),
            pltpu.VMEM((8, 8, 16, HID), BF16),
            pltpu.VMEM((ROWS, D), BF16),
            pltpu.VMEM((HID, ROWS), BF16),
            pltpu.VMEM((COLS, ROWS), F32),
            pltpu.VMEM((8, 2, 16, ROWS), F32),
            pltpu.VMEM((8, 8, ROWS), F32),
            pltpu.VMEM((32, 704), BF16),
            pltpu.VMEM((32, 704), BF16),
            pltpu.VMEM((32, 704), BF16),
            pltpu.VMEM((1, D), F32),
            pltpu.VMEM((128, 128), BF16),
            pltpu.VMEM((1, 128), F32),
            pltpu.VMEM((1, D), F32),
            *scatter_scratch(ROWS, COLS),
            *scatter_scratch(128, ROWS),
            *scatter_scratch(128, ROWS),
            pltpu.VMEM((3072, 128), BF16),
            pltpu.SemaphoreType.DMA((10,)),
            pltpu.SemaphoreType.DMA((SENDING,)),
            pltpu.SemaphoreType.DMA((ARRIVALS,)),
        ],
        compiler_params=pltpu.CompilerParams(
            collective_id=0, has_side_effects=True, vmem_limit_bytes=67043328
        ),
        name="layer",
    )(
        tokens, pool_input, pool_output.T, gate_weight, up_weight, down_weight.T, mixer_gain.reshape(1, D), group_weight.reshape(128, 128), channel_scale.reshape(1, 128),
        ffn_gain.reshape(1, D),
    )
    return (scaled * final_gain).astype(BF16)


def solution(mesh):
    torus = Mesh(mesh.devices.reshape(8, 8, 4, 2), ("z", "y", "x", "c"))
    in_specs = (
        P(FS, TP),
        P(),
        P(FS, TP),
        P(TP, None, None),
        P(TP),
        P(TP, FS),
        P(),
        P(FS, TP),
        P(FS, TP),
        P(TP, FS),
        P(TP),
    )
    return jax.shard_map(local, mesh=torus, in_specs=in_specs, out_specs=P(FS, TP), check_vma=False)
```

```python
import jax
import jax.numpy as jnp
from jax import lax
from jax.experimental import pallas as pl
from jax.experimental.pallas import tpu as pltpu
from jax.sharding import Mesh
from jax.sharding import PartitionSpec as P

MESH = pl.DeviceIdType.MESH
F32 = jnp.float32
BF16 = jnp.bfloat16
D = 2048
ROWS = 384
COLS = 256
LENGTH = 128
HID = 768
FS = ("z", "y")
TP = ("x", "c")
EPS = 1e-06
SENDING = 96
ARRIVALS = 90

STREAMS = (
    ("PI", 0, 128, 16), ("PO", 0, 128, 16), ("G", 0, 384, 16), ("G", 384, 256, 16), ("G", 640, 256, 16),
    ("G", 896, 256, 16), ("G", 1152, 256, 16), ("D0", 0, 384, 16), ("D1", 0, 384, 16),
)
DIRECT = (0, 1)
LINK = {1: (46.6e3, 2.9), -1: (46.6e3, 2.9), "x": (46.6e3, 2.9), "d": (500e3, 1.5)}
WINDOW = 3
FAR = 2.9
MIX, GATES, DOWN = (0, 1), (2, 3, 4, 5, 6), (7, 8)


def hops(stream, phase, sign):
    return 4 if phase == 2 or (stream % 2 == 0) == (sign > 0) else 3


def tile_streams(i):
    return [s for s in GATES if STREAMS[s][1] < 256 * i + 256 and STREAMS[s][1] + STREAMS[s][2] > 256 * i]


def events():
    plan = []

    def add(name, rank, needs=(), after=(), cost=0.1, sends=()):
        plan.append((name, rank, tuple(needs), tuple(after), cost, tuple(sends)))

    for s, (_, first, lanes, rows) in enumerate(STREAMS):
        piece = 2 * rows * lanes
        if s in DIRECT:
            add(("w", s, 0, 4), s - 20, sends=[(("w", s, 1, 4), sign, 8 * piece) for sign in (1, -1)])
        for phase in (1, 2):
            for k in range(1, 5):
                if phase == 1 and s in DIRECT:
                    continue
                needs = [("w", s, phase, k - 1)] if k > 1 else [("w", s, 1, 4)] if phase == 2 else []
                after = [("w", s - WINDOW, 2, 2)] if phase == 2 and k == 1 and s >= WINDOW else []
                size = piece * (8 if phase == 2 else 1)
                cost = 0.05 if phase == 2 else 0.15
                size = size // 2 if (phase, k) == (2, 4) else size
                sends = [(("w", s, phase, k), sign, size) for sign in (1, -1) if k <= hops(s, phase, sign)]
                add(("w", s, phase, k), s - 10, needs, after, cost, sends)

    def add_gather(tag, rank, first):
        half, over = ROWS * COLS, lambda *keys: [((tag, "d", k), "d", ROWS * COLS) for k in keys]
        sends = [((tag, "near"), "x", half), ((tag, "next"), "x", half), ((tag, "own"), "d", 2 * half)]
        add((tag, 0), rank, [], first, 0.1, sends)
        add((tag, 1), rank, [(tag, "near")], [(tag, 0)], 0.1, [((tag, "far"), "x", half)] + over(0, 1))
        add((tag, 2), rank, [(tag, "next")], [(tag, 1)], 0.1, over(2, 3))
        add((tag, 3), rank, [(tag, "far")], [(tag, 2)], 0.1, over(4, 5))
        add((tag, 4), rank, [(tag, "own")] + [(tag, "d", k) for k in range(6)], [(tag, 3)])

    def add_scatter(tag, rank, source, block):
        half = block // 2
        add((tag, 1), rank, [(tag, "q", 2)], [source], 0.15, [((tag, "far"), "x", half)])
        add((tag, 2), rank, [(tag, "q", 1), (tag, "q", -1)], [(tag, 1)], 0.15, [((tag, "one"), "x", half)])
        add((tag, 3), rank, [(tag, "far")], [(tag, 2)], 0.15, [((tag, "two"), "x", half)])

    def whole(tag):
        return [(tag, "two"), (tag, "one"), (tag, "q", 0)]

    block1, block2 = 2 * ROWS * COLS, 2 * ROWS * 128
    add_gather("g1", -30, [])
    add("norm1", 0, [], [("g1", 4)], 0.7)
    add("mixer", 0, [("w", s, 2, 4) for s in MIX], ["norm1"], 2.0, [(("s1", "q", o), "d", block1) for o in (2, 1, -1, 0)])
    add_scatter("s1", -5, "mixer", block1)
    add_gather("g2", -5, ["middle"])
    add("middle", 0, whole("s1"), [("s1", 3)], 0.8)
    add("norm2", 0, [], [("g2", 4)], 0.7)
    for i in range(6):
        add(("h", i), 0, [("w", s, 2, 4) for s in tile_streams(i)], [("h", i - 1)] if i else ["norm2"], 1.06)
    for h in range(2):
        tag, before = f"s{2 + h}", ("h", 5)
        for offset in (2, 1, -1, 0):
            name = ("d", h, offset)
            add(name, h, [("w", DOWN[h], 2, 4)], [before], 0.4, [((tag, "q", offset), "d", block2)])
            before = name
        add_scatter(tag, h - 3, ("d", h, 2), block2)
        add(("c", h), h - 3, whole(tag), [(tag, 3)], 0.4)
    add("last", 9, [], [("c", 0), ("c", 1)], 4.0)
    return plan


def order(plan, margin=0.3):
    now, free, arrival, done, left, result = 0.0, {}, {}, set(), list(plan), []
    while left:
        best = None
        for e in left:
            name, rank, needs, after, cost, sends = e
            if any(k not in arrival for k in needs) or any(k not in done for k in after):
                continue
            key = (max([now] + [arrival[k] + margin for k in needs]), rank)
            if best is None or key < best[0]:
                best = (key, e)
        (ready, _), e = best
        name, rank, needs, after, cost, sends = e
        now = ready + cost
        done.add(name)
        for key, link, size in sends:
            rate, delay = LINK[link]
            free[link] = max(free.get(link, 0.0), now) + size / rate
            arrival[key] = max(arrival.get(key, 0.0), free[link] + delay + (FAR if name[:1] == ("w",) and name[2] == 0 else 0.0))
        left.remove(e)
        result.append((ready, name))
    return result


def kernel(
    tok, pool_in, pool_out, gate, up, down_t, mixer_gain_in, group_weight_in, channel_scale_in, ffn_gain_in,
    final_gain_in, out,
    T, M, PIN, POUT, GU, DN0, DN1, N, HT, MT, C, SQ,
    gate_own, up_own, down_own, mixer_gain, group_weight, channel_scale, ffn_gain, final_gain,
    S1, Q1, U1, RL1, F1, S2, Q2, U2, RL2, F2, S3, Q3, U3, RL3, F3, W,
    local_sem, send_sem, recv_sem,
):
    z, y, x, c = (lax.axis_index(n) for n in ("z", "y", "x", "c"))
    me = 2 * x + c
    DN = (DN0, DN1)
    place = {"z": z, "y": y, "x": x, "c": c}
    size = {"z": 8, "y": 8, "x": 4, "c": 2}

    def near(axis, offset):
        return lax.rem(place[axis] + (offset + size[axis]), size[axis])

    def at(axis, offset):
        return {axis: near(axis, offset)}

    barrier = pltpu.get_barrier_semaphore()
    friends = [at(axis, o) for axis in ("y", "z") for o in (1, -1, 2, -2, 3, -3, 4)]
    peers = [{"x": near("x", dx), "c": near("c", dc)} for dx in range(4) for dc in range(2) if (dx, dc) != (0, 0)]
    for friend in friends + peers:
        pl.semaphore_signal(barrier, inc=1, device_id=friend, device_id_type=MESH)
    local_copies = [
        (gate, gate_own), (up, up_own), (down_t, down_own), (pool_in, PIN.at[z, y]), (pool_out, POUT.at[z, y]),
        (tok, T.at[me]), (mixer_gain_in, mixer_gain), (group_weight_in, group_weight),
        (channel_scale_in, channel_scale), (ffn_gain_in, ffn_gain), (final_gain_in, final_gain),
    ]
    local_copies = [pltpu.make_async_copy(a, b, local_sem.at[i]) for i, (a, b) in enumerate(local_copies)]
    for copy in local_copies:
        copy.start()

    for copy in local_copies:
        copy.wait()
    for i in range(5):
        GU[z, y, :, 256 * i : 256 * i + 128] = gate_own[:, 128 * i : 128 * i + 128]
        GU[z, y, :, 256 * i + 128 : 256 * i + 256] = up_own[:, 128 * i : 128 * i + 128]
    GU[z, y, :, 1280:1408] = jnp.concatenate([gate_own[:, 640:], up_own[:, 640:]], axis=1)
    padded = jnp.concatenate([down_own[:, 640:], jnp.zeros((32, 64), BF16)], axis=1)
    for h in range(2):
        DN[h][z, y, :, :640] = down_own[16 * h : 16 * h + 16, :640]
        DN[h][z, y, :, 640:] = padded[16 * h : 16 * h + 16]
    pl.semaphore_wait(barrier, len(friends) + len(peers))

    sent, groups = [], {}

    def send(src, dst, device, group):
        i = len(sent)
        if i >= SENDING:
            sent[i - SENDING].wait_send()
        slot, size = groups.setdefault(group, (len(groups), 0))
        bytes_of = dst.dtype.itemsize
        for n in dst.shape:
            bytes_of *= n
        groups[group] = (slot, size + bytes_of)
        copy = pltpu.make_async_remote_copy(
            src_ref=src, dst_ref=dst, send_sem=send_sem.at[i % SENDING], recv_sem=recv_sem.at[slot],
            device_id=device, device_id_type=MESH,
        )
        copy.start()
        sent.append(copy)

    def arrived(group):
        slot, size = groups[group]
        ref = W.at[pl.ds(0, size // 256)]
        pltpu.make_async_copy(ref, ref, recv_sem.at[slot]).wait()

    def part(s, route, zi, yi):
        name, first, lanes, rows = STREAMS[s]
        if name[0] == "D":
            ref, tail = DN[int(name[1])], (slice(None), pl.ds(384 * route, 384))
        else:
            ref = {"PI": PIN, "PO": POUT, "G": GU}[name]
            tail = (pl.ds(16 * route, 16), pl.ds(first, lanes))
        return ref.at[(zi, yi) + tail]

    def slab(s, route, phase, origin, whole=slice(None)):
        if phase == 1:
            return part(s, route, z, origin) if route == 0 else part(s, route, origin, y)
        return part(s, route, origin, whole) if route == 0 else part(s, route, whole, origin)

    def spread(s):
        for route in range(2):
            axis = "yz"[route]
            ref = slab(s, route, 1, place[axis])
            for offset in (1, -1, 2, -2, 3, -3, 4):
                send(ref, ref, at(axis, offset), ("w", s, 1, 4))

    def step(s, phase, k):
        if k > 1:
            arrived(("w", s, phase, k - 1))
        elif phase == 2:
            arrived(("w", s, 1, 4))
        for route in range(2):
            axis = "y" if (route == 0) == (phase == 1) else "z"
            for sign in (1, -1):
                if k <= hops(s, phase, sign):
                    pieces = slice(None) if (phase, k) != (2, 4) else slice(0, 4) if sign > 0 else slice(4, 8)
                    ref = slab(s, route, phase, near(axis, -sign * (k - 1)), pieces)
                    send(ref, ref, at(axis, sign), ("w", s, phase, k))

    def finish(s):
        arrived(("w", s, 2, 4))

    def gather(B, tag):
        lo, hi = slice(0, ROWS // 2), slice(ROWS // 2, ROWS)
        right, left, other = at("x", 1), at("x", -1), at("c", 1)
        from_left, from_right, across = (2 * near("x", o) + c for o in (-1, 1, 2))

        def pass_on(block, half, device, group):
            ref = B.at[block, half]
            send(ref, ref, device, (tag, group))

        def start():
            pass_on(me, lo, right, "near")
            pass_on(me, hi, left, "near")
            pass_on(me, hi, right, "next")
            pass_on(me, lo, left, "next")
            send(B.at[me], B.at[me], other, (tag, "d"))

        def relay():
            arrived((tag, "near"))
            pass_on(from_left, lo, right, "far")
            pass_on(from_right, hi, left, "far")
            pass_on(from_left, lo, other, "d")
            pass_on(from_right, hi, other, "d")

        def rest():
            arrived((tag, "next"))
            pass_on(from_left, hi, other, "d")
            pass_on(from_right, lo, other, "d")

        def far():
            arrived((tag, "far"))
            pass_on(across, lo, other, "d")
            pass_on(across, hi, other, "d")

        def end():
            arrived((tag, "d"))

        return start, relay, rest, far, end

    def scatter(S, Q, U, RL, F, tag):
        n = S.shape[2]
        lo, hi = slice(0, n // 2), slice(n // 2, n)
        right, left, other = at("x", 1), at("x", -1), at("c", 1)

        def hand_over(offset):
            b = near("x", offset)
            send(S.at[b, near("c", 1)], Q.at[b], other, (tag, "q", abs(offset)))

        def pair(offset, half):
            b = near("x", offset)
            return S[b, c, half, :].astype(F32) + Q[b, half, :].astype(F32)

        def first():
            arrived((tag, "q", 2))
            U[2, lo, :] = pair(2, lo).astype(BF16)
            send(U.at[2, lo], RL.at[lo], right, (tag, "far"))
            U[2, hi, :] = pair(2, hi).astype(BF16)
            send(U.at[2, hi], RL.at[hi], left, (tag, "far"))

        def second():
            arrived((tag, "q", 1))
            U[0, hi, :] = pair(1, hi).astype(BF16)
            send(U.at[0, hi], F.at[0, hi], right, (tag, "near"))
            U[1, lo, :] = pair(-1, lo).astype(BF16)
            send(U.at[1, lo], F.at[1, lo], left, (tag, "near"))

        def third():
            arrived((tag, "far"))
            U[0, lo, :] = (pair(1, lo) + RL[lo, :].astype(F32)).astype(BF16)
            send(U.at[0, lo], F.at[0, lo], right, (tag, "near"))
            U[1, hi, :] = (pair(-1, hi) + RL[hi, :].astype(F32)).astype(BF16)
            send(U.at[1, hi], F.at[1, hi], left, (tag, "near"))

        def total():
            arrived((tag, "q", 0))
            arrived((tag, "near"))
            return pair(0, slice(0, n)) + F[0].astype(F32) + F[1].astype(F32)

        return hand_over, first, second, third, total

    def norm(B, gain):
        def rows_of(i, carry):
            rows = pl.ds(pl.multiple_of(i * 128, 128), 128)
            squares = jnp.zeros((128, COLS), F32)
            for j in range(8):
                v = B[j, rows, :].astype(F32)
                squares = squares + v * v
            r = lax.rsqrt(jnp.sum(squares, axis=1, keepdims=True) * (1.0 / D) + EPS)
            for j in range(8):
                lanes = slice(COLS * j, COLS * j + COLS)
                N[rows, lanes] = (B[j, rows, :].astype(F32) * r * gain[:, lanes]).astype(BF16)
            return carry

        lax.fori_loop(0, 3, rows_of, 0)

    gather1, gather2 = gather(T, "g1"), gather(M, "g2")
    scatter1 = scatter(S1, Q1, U1, RL1, F1, "s1")
    scatters = (scatter(S2, Q2, U2, RL2, F2, "s2"), scatter(S3, Q3, U3, RL3, F3, "s3"))

    def mixer():
        for s in MIX:
            finish(s)
        pooled_in = jnp.dot(N[...], PIN[...].reshape(D, 128), preferred_element_type=F32).astype(BF16)
        window = jnp.left_shift(jnp.int32(2), lax.rem(me, 4))
        later = lax.broadcasted_iota(jnp.int32, (LENGTH, LENGTH), 0)
        earlier = lax.broadcasted_iota(jnp.int32, (LENGTH, LENGTH), 1)
        inside = (earlier <= later) & (earlier > later - window)
        band = jnp.where(inside, 1.0, 0.0).astype(BF16)
        divisor = jnp.minimum(later + 1, window).astype(F32)
        grouped = []
        for s in range(ROWS // LENGTH):
            own = pooled_in[s * LENGTH : (s + 1) * LENGTH]
            sums = jnp.dot(band, own, preferred_element_type=F32)
            pooled = (sums / divisor - own.astype(F32)).astype(BF16)
            mapped = jnp.dot(pooled, group_weight[...], preferred_element_type=F32)
            grouped.append((mapped * channel_scale[...]).astype(BF16))
        grouped = jnp.concatenate(grouped, axis=0)
        for offset in (2, 1, -1, 0):
            b = near("x", offset)
            for core in (near("c", 1), c):
                piece = POUT[2 * b + core].reshape(COLS, 128)
                terms = lax.dot_general(grouped, piece, (((1,), (1,)), ((), ())), preferred_element_type=F32)
                S1[b, core] = terms.astype(BF16)
            scatter1[0](offset)

    def middle():
        value = (T[me].astype(F32) + scatter1[4]()).astype(BF16)
        M[me] = value
        gather2[0]()
        MT[...] = jnp.transpose(value.astype(F32))

    def silu_up(g, u):
        return g / (1.0 + jnp.exp(-g)) * u

    settled = set()

    def settle(i):
        for s in tile_streams(i):
            if s not in settled:
                finish(s)
                settled.add(s)

    def hidden(i):
        settle(i)
        piece = GU[:, :, :, 256 * i : 256 * i + 256].reshape(D, 256)
        acc = jnp.dot(N[...], piece, preferred_element_type=F32)
        h = silu_up(acc[:, :128], acc[:, 128:])
        HT[128 * i : 128 * i + 128, :] = jnp.transpose(h).astype(BF16)

    def hidden_tail():
        settle(5)
        acc = jnp.dot(N[...], GU[:, :, :, 1280:1408].reshape(D, 128), preferred_element_type=F32)
        h = silu_up(acc, pltpu.roll(acc, 64, 1))
        lane = lax.broadcasted_iota(jnp.int32, h.shape, 1)
        HT[640:768, :] = jnp.transpose(jnp.where(lane < 64, h, 0.0)).astype(BF16)

    def down(h, S, offset):
        if offset == 2:
            finish(DOWN[h])
        b = near("x", offset)
        piece = DN[h][pl.ds(2 * b, 2)].reshape(256, HID)
        terms = jnp.dot(piece, HT[...], preferred_element_type=F32).astype(BF16)
        S[b] = terms.reshape(2, 128, ROWS)
        scatters[h][0](offset)

    def collect(h):
        C[:, h] = scatters[h][4]().reshape(8, 16, ROWS)

    def last():
        C[...] = C[...] + MT[...].reshape(8, 2, 16, ROWS)
        closing = C[...].reshape(COLS, ROWS)
        own = jnp.sum(closing * closing, axis=0, keepdims=True)
        SQ[me] = jnp.broadcast_to(own, (8, ROWS))
        for peer in peers:
            send(SQ.at[me], SQ.at[me], peer, "squares")
        arrived("squares")
        squares = jnp.sum(SQ[...], axis=0)[0:1]
        scaled = C[...].reshape(COLS, ROWS) * lax.rsqrt(squares * (1.0 / D) + EPS)
        out[...] = (jnp.transpose(scaled) * final_gain[...]).astype(BF16)

    runs = {"norm1": lambda: norm(T, mixer_gain), "mixer": mixer, "middle": middle, "norm2": lambda: norm(M, ffn_gain)}
    for s in range(len(STREAMS)):
        runs["w", s, 0, 4] = lambda s=s: spread(s)
        for phase in (1, 2):
            for k in range(1, 5):
                runs["w", s, phase, k] = lambda s=s, phase=phase, k=k: step(s, phase, k)
    for tag, parts in (("g1", gather1), ("g2", gather2), ("s1", scatter1), ("s2", scatters[0]), ("s3", scatters[1])):
        for i, part_run in enumerate(parts):
            runs[tag, i] = part_run
    runs["g2", 0] = lambda: None
    for i in range(5):
        runs["h", i] = lambda i=i: hidden(i)
    runs["h", 5] = hidden_tail
    for h, S in enumerate((S2, S3)):
        runs["c", h] = lambda h=h: collect(h)
        for offset in (2, 1, -1, 0):
            runs["d", h, offset] = lambda h=h, S=S, offset=offset: down(h, S, offset)
    runs["last"] = last
    for t, name in order(events()):
        runs[name]()
    for copy in sent[-SENDING:]:
        copy.wait_send()


def scatter_scratch(n, lanes):
    return [
        pltpu.VMEM((4, 2, n, lanes), BF16),
        pltpu.VMEM((4, n, lanes), BF16),
        pltpu.VMEM((3, n, lanes), BF16),
        pltpu.VMEM((n, lanes), BF16),
        pltpu.VMEM((2, n, lanes), BF16),
    ]


def local(
    tokens, mixer_gain, pool_input, group_weight, channel_scale, pool_output,
    ffn_gain, gate_weight, up_weight, down_weight, final_gain,
):
    vmem = pl.BlockSpec(memory_space=pltpu.VMEM)
    hbm = pl.BlockSpec(memory_space=pltpu.HBM)
    operands = (
        tokens, pool_input, pool_output.T, gate_weight, up_weight, down_weight.T, mixer_gain.reshape(1, D),
        group_weight.reshape(128, 128), channel_scale.reshape(1, 128), ffn_gain.reshape(1, D), final_gain.reshape(1, COLS),
    )
    return pl.pallas_call(
        kernel,
        out_shape=jax.ShapeDtypeStruct((ROWS, COLS), BF16),
        in_specs=[hbm] * 11,
        out_specs=vmem,
        scratch_shapes=[
            pltpu.VMEM((8, ROWS, COLS), BF16),
            pltpu.VMEM((8, ROWS, COLS), BF16),
            pltpu.VMEM((8, 8, 32, 128), BF16),
            pltpu.VMEM((8, 8, 32, 128), BF16),
            pltpu.VMEM((8, 8, 32, 1408), BF16),
            pltpu.VMEM((8, 8, 16, HID), BF16),
            pltpu.VMEM((8, 8, 16, HID), BF16),
            pltpu.VMEM((ROWS, D), BF16),
            pltpu.VMEM((HID, ROWS), BF16),
            pltpu.VMEM((COLS, ROWS), F32),
            pltpu.VMEM((8, 2, 16, ROWS), F32),
            pltpu.VMEM((8, 8, ROWS), F32),
            pltpu.VMEM((32, 704), BF16),
            pltpu.VMEM((32, 704), BF16),
            pltpu.VMEM((32, 704), BF16),
            pltpu.VMEM((1, D), F32),
            pltpu.VMEM((128, 128), BF16),
            pltpu.VMEM((1, 128), F32),
            pltpu.VMEM((1, D), F32),
            pltpu.VMEM((1, COLS), F32),
            *scatter_scratch(ROWS, COLS),
            *scatter_scratch(128, ROWS),
            *scatter_scratch(128, ROWS),
            pltpu.VMEM((3072, 128), BF16),
            pltpu.SemaphoreType.DMA((11,)),
            pltpu.SemaphoreType.DMA((SENDING,)),
            pltpu.SemaphoreType.DMA((ARRIVALS,)),
        ],
        compiler_params=pltpu.CompilerParams(
            collective_id=0, has_side_effects=True, vmem_limit_bytes=50 * 1024 * 1024
        ),
        name="layer",
    )(*(pltpu.with_memory_space_constraint(a, pltpu.HBM) for a in operands))


def solution(mesh):
    torus = Mesh(mesh.devices.reshape(8, 8, 4, 2), ("z", "y", "x", "c"))
    in_specs = (
        P(FS, TP),
        P(),
        P(FS, TP),
        P(TP, None, None),
        P(TP),
        P(TP, FS),
        P(),
        P(FS, TP),
        P(FS, TP),
        P(TP, FS),
        P(TP),
    )
    return jax.shard_map(local, mesh=torus, in_specs=in_specs, out_specs=P(FS, TP), check_vma=False)
```

```python
import jax
import jax.numpy as jnp
from jax import lax
from jax.experimental import pallas as pl
from jax.experimental.pallas import tpu as pltpu
from jax.sharding import Mesh
from jax.sharding import PartitionSpec as P

MESH = pl.DeviceIdType.MESH
F32 = jnp.float32
BF16 = jnp.bfloat16
D = 2048
ROWS = 384
COLS = 256
LENGTH = 128
HID = 768
FS = ("z", "y")
TP = ("x", "c")
EPS = 1e-06
SENDING = 32
ARRIVALS = 82

STREAMS = (
    ("PI", 0, 128, 16), ("PO", 0, 128, 16),
    ("G", 0, 512, 16),
    ("G", 512, 512, 16),
    ("G", 1024, 256, 16),
    ("G", 1280, 128, 16),
    ("D0", 0, 384, 16),
    ("D1", 0, 384, 16),
)
DIRECT = (0, 1)
LINK = {1: (46.6e3, 2.9), -1: (46.6e3, 2.9), "x": (46.6e3, 2.7), "d": (500e3, 1.1)}
WINDOW = 3
EARLY = (2, 3)
FAR = 2.9
MIXER, CHAIN = -20, -20
MIX, GATES, DOWN = (0, 1), (2, 3, 4, 5), (6, 7)
DOWN_ROWS = ((0, 16), (16, 16))


def hops(stream, phase, sign):
    return 4 if phase == 2 or (stream % 2 == 0) == (sign > 0) else 3


def ahead(k):
    return (0,) if k == 1 else (k - 1, 1 - k)


def tile_streams(i):
    return [s for s in GATES if STREAMS[s][1] < 256 * i + 256 and STREAMS[s][1] + STREAMS[s][2] > 256 * i]


def events():
    plan = []

    def add(name, rank, needs=(), after=(), cost=0.1, sends=()):
        plan.append((name, rank, tuple(needs), tuple(after), cost, tuple(sends)))

    for s, (_, first, lanes, rows) in enumerate(STREAMS):
        piece = 2 * rows * lanes
        if s in DIRECT:
            add(("w", s, 0, 4), s - 20, sends=[(("w", s, 1, 4), sign, 8 * piece) for sign in (1, -1)])
        for phase in (1, 2):
            for k in range(1, 5):
                if phase == 1 and s in DIRECT:
                    continue
                needs = [("w", s, phase, k - 1)] if k > 1 else [("w", s, 1, 4)] if phase == 2 else []
                after = [("w", s - WINDOW, 2, 2)] if phase == 2 and k == 1 and s >= WINDOW and s not in EARLY else []
                after += [("w", s, 2, 1)] if (phase, k) == (2, 2) else []
                size = piece * (8 if phase == 2 else 1)
                cost = 0.05 if phase == 2 else 0.15
                size = size // 2 if (phase, k) == (2, 4) else size
                if s in EARLY and (phase, k) == (2, 1):
                    size = piece
                sends = [(("w", s, phase, k), sign, size) for sign in (1, -1) if k <= hops(s, phase, sign)]
                if s in EARLY and phase == 1:
                    sends += [(("w", s, 2, 1), sign, piece * len(ahead(k))) for sign in (1, -1)]
                add(("w", s, phase, k), s - 10, needs, after, cost, sends)

    def add_gather(tag, rank, first):
        half, over = ROWS * COLS, lambda *keys: [((tag, "d", k), "d", ROWS * COLS) for k in keys]
        sends = [((tag, "near"), "x", half), ((tag, "next"), "x", half), ((tag, "own"), "d", 2 * half)]
        add((tag, 0), rank, [], first, 0.1, sends)
        add((tag, 1), rank, [(tag, "near")], [(tag, 0)], 0.1, [((tag, "far"), "x", half)] + over(0, 1))
        add((tag, 2), rank, [(tag, "next")], [(tag, 1)], 0.1, over(2, 3))
        add((tag, 3), rank, [(tag, "far")], [(tag, 2)], 0.1, over(4, 5))
        add((tag, 4), rank, [(tag, "own")] + [(tag, "d", k) for k in range(6)], [(tag, 3)])

    def add_scatter(tag, rank, source, block):
        half = block // 2
        add((tag, 1), rank, [(tag, "q", 2)], [source], 0.1, [((tag, "far"), "x", half)])
        add((tag, 2), rank + 0, [(tag, "q", 1), (tag, "q", -1)], [(tag, 1)] + (["mixer1"] if tag == "s1" else []), 0.1, [((tag, "one"), "x", half)])
        add((tag, 3), rank, [(tag, "far")], [(tag, 2)], 0.1, [((tag, "two"), "x", half)])

    def whole(tag):
        return [(tag, "two"), (tag, "one"), (tag, "q", 0)]

    block1 = 2 * ROWS * COLS
    add_gather("g1", -30, [])
    add("norm1", 0, [], [("g1", 4)], 0.7)
    add("mixer", MIXER, [("w", s, 2, 4) for s in MIX], ["norm1"], 2.0, [(("s1", "q", 2), "d", block1)])
    add("mixer1", MIXER, [], ["mixer"], 0.9, [(("s1", "q", o), "d", block1) for o in (1, -1)])
    add("mixer2", MIXER, [], ["mixer1"], 0.5, [(("s1", "q", 0), "d", block1)])
    add_scatter("s1", CHAIN, "mixer", block1)
    add_gather("g2", CHAIN, ["middle"])
    add("middle", CHAIN, whole("s1"), [("s1", 3), "mixer2"], 0.4)
    add("norm2", 0, [], [("g2", 4)], 0.7)
    for i in range(6):
        add(("h", i), 0, [("w", s, 2, 4) for s in tile_streams(i)], [("h", i - 1)] if i else ["norm2"], 1.06)
    for h, (_, rows) in enumerate(DOWN_ROWS):
        tag, before, block2 = f"s{2 + h}", ("h", 5), 2 * ROWS * 8 * rows
        for offset in (2, 1, -1, 0):
            name = ("d", h, offset)
            add(name, h, [("w", DOWN[h], 2, 4)], [before], 0.17 + 0.0125 * rows, [((tag, "q", offset), "d", block2)])
            before = name
        add_scatter(tag, h - 4, ("d", h, 2), block2)
        add(("c", h), h - 4, whole(tag), [(tag, 3)], 0.025 * rows)
    add("last", 9, [], [("c", h) for h in range(len(DOWN))], 4.0)
    return plan


def order(plan, margin=0.15):
    now, free, arrival, done, left, result = 0.0, {}, {}, set(), list(plan), []
    while left:
        best = None
        for e in left:
            name, rank, needs, after, cost, sends = e
            if any(k not in arrival for k in needs) or any(k not in done for k in after):
                continue
            key = (max([now] + [arrival[k] + margin for k in needs]), rank)
            if best is None or key < best[0]:
                best = (key, e)
        (ready, _), e = best
        name, rank, needs, after, cost, sends = e
        now = ready + cost
        done.add(name)
        for key, link, size in sends:
            rate, delay = LINK[link]
            free[link] = max(free.get(link, 0.0), now) + size / rate
            arrival[key] = max(arrival.get(key, 0.0), free[link] + delay + (FAR if name[:1] == ("w",) and name[2] == 0 else 0.0))
        left.remove(e)
        result.append((ready, name))
    return result


def kernel(
    tok, pool_in, pool_out, gate, up, down_t, mixer_gain_in, group_weight_in, channel_scale_in, ffn_gain_in,
    final_gain_in, out,
    T, M, PIN, POUT, GU, DN0, DN1, N, GR, HT, MT, C, SQ,
    gate_own, up_own, down_own, mixer_gain, group_weight, channel_scale, ffn_gain, final_gain,
    S1, Q1, U1, RL1, F1, S2, Q2, U2, RL2, F2, S3, Q3, U3, RL3, F3, W,
    local_sem, send_sem, recv_sem,
):
    z, y, x, c = (lax.axis_index(n) for n in ("z", "y", "x", "c"))
    me = 2 * x + c
    DN = (DN0, DN1)
    place = {"z": z, "y": y, "x": x, "c": c}
    size = {"z": 8, "y": 8, "x": 4, "c": 2}

    def near(axis, offset):
        return lax.rem(place[axis] + (offset + size[axis]), size[axis])

    def at(axis, offset):
        return {axis: near(axis, offset)}

    barrier = pltpu.get_barrier_semaphore()
    friends = [at(axis, o) for o in (4, 3, -3, 2, -2, 1, -1) for axis in ("z", "y")]
    peers = [{"x": near("x", dx), "c": near("c", dc)} for dx in range(4) for dc in range(2) if (dx, dc) != (0, 0)]
    for friend in friends + peers:
        pl.semaphore_signal(barrier, inc=1, device_id=friend, device_id_type=MESH)
    local_copies = [
        (gate, gate_own), (up, up_own), (down_t, down_own), (pool_in, PIN.at[z, y]), (pool_out, POUT.at[z, y]),
        (tok, T.at[me]), (mixer_gain_in, mixer_gain), (group_weight_in, group_weight),
        (channel_scale_in, channel_scale), (ffn_gain_in, ffn_gain), (final_gain_in, final_gain),
    ]
    local_copies = [pltpu.make_async_copy(a, b, local_sem.at[i]) for i, (a, b) in enumerate(local_copies)]
    for copy in local_copies:
        copy.start()

    for copy in local_copies:
        copy.wait()
    for i in range(5):
        GU[z, y, :, 256 * i : 256 * i + 128] = gate_own[:, 128 * i : 128 * i + 128]
        GU[z, y, :, 256 * i + 128 : 256 * i + 256] = up_own[:, 128 * i : 128 * i + 128]
    GU[z, y, :, 1280:1408] = jnp.concatenate([gate_own[:, 640:], up_own[:, 640:]], axis=1)
    padded = jnp.concatenate([down_own[:, 640:], jnp.zeros((32, 64), BF16)], axis=1)
    for h, (first, rows) in enumerate(DOWN_ROWS):
        DN[h][z, y, :, :640] = down_own[first : first + rows, :640]
        DN[h][z, y, :, 640:] = padded[first : first + rows]
    pl.semaphore_wait(barrier, len(friends) + len(peers))

    leaving, groups, turn = [0] * SENDING, {}, [0]

    def drain(slot):
        if leaving[slot]:
            ref = W.at[pl.ds(0, leaving[slot] // 256)]
            pltpu.make_async_copy(ref, ref, send_sem.at[slot]).wait()
            leaving[slot] = 0

    def next_event():
        turn[0] = (turn[0] + 1) % SENDING
        drain(turn[0])

    def send(src, dst, device, group):
        slot, size = groups.setdefault(group, (len(groups), 0))
        bytes_of = dst.dtype.itemsize
        for n in dst.shape:
            bytes_of *= n
        groups[group] = (slot, size + bytes_of)
        leaving[turn[0]] += bytes_of
        pltpu.make_async_remote_copy(
            src_ref=src, dst_ref=dst, send_sem=send_sem.at[turn[0]], recv_sem=recv_sem.at[slot],
            device_id=device, device_id_type=MESH,
        ).start()

    def arrived(group):
        slot, size = groups[group]
        ref = W.at[pl.ds(0, size // 256)]
        pltpu.make_async_copy(ref, ref, recv_sem.at[slot]).wait()

    def part(s, route, zi, yi):
        name, first, lanes, rows = STREAMS[s]
        if name[0] == "D":
            ref, tail = DN[int(name[1])], (slice(None), pl.ds(384 * route, 384))
        else:
            ref = {"PI": PIN, "PO": POUT, "G": GU}[name]
            tail = (pl.ds(16 * route, 16), pl.ds(first, lanes))
        return ref.at[(zi, yi) + tail]

    def slab(s, route, phase, origin, whole=slice(None)):
        if phase == 1:
            return part(s, route, z, origin) if route == 0 else part(s, route, origin, y)
        return part(s, route, origin, whole) if route == 0 else part(s, route, whole, origin)

    def spread(s):
        for route in range(2):
            axis = "yz"[route]
            ref = slab(s, route, 1, place[axis])
            for offset in (1, -1, 2, -2, 3, -3, 4):
                send(ref, ref, at(axis, offset), ("w", s, 1, 4))

    def send_ahead(s, offsets):
        for route in range(2):
            for sign in (1, -1):
                for offset in offsets:
                    ref = slab(s, route, 1, near("yz"[route], offset))
                    send(ref, ref, at("zy"[route], sign), ("w", s, 2, 1))

    def step(s, phase, k):
        if k > 1:
            arrived(("w", s, phase, k - 1))
        elif phase == 2:
            arrived(("w", s, 1, 4))
        if s in EARLY and (phase, k) == (2, 1):
            send_ahead(s, (4,))
            return
        for route in range(2):
            axis = "y" if (route == 0) == (phase == 1) else "z"
            for sign in (1, -1):
                if k <= hops(s, phase, sign):
                    pieces = slice(None) if (phase, k) != (2, 4) else slice(0, 4) if sign > 0 else slice(4, 8)
                    ref = slab(s, route, phase, near(axis, -sign * (k - 1)), pieces)
                    send(ref, ref, at(axis, sign), ("w", s, phase, k))
        if s in EARLY and phase == 1:
            send_ahead(s, ahead(k))

    def finish(s):
        arrived(("w", s, 2, 4))

    def gather(B, tag):
        lo, hi = slice(0, ROWS // 2), slice(ROWS // 2, ROWS)
        right, left, other = at("x", 1), at("x", -1), at("c", 1)
        from_left, from_right, across = (2 * near("x", o) + c for o in (-1, 1, 2))

        def pass_on(block, half, device, group):
            ref = B.at[block, half]
            send(ref, ref, device, (tag, group))

        def start():
            pass_on(me, lo, right, "near")
            pass_on(me, hi, left, "near")
            pass_on(me, hi, right, "next")
            pass_on(me, lo, left, "next")
            send(B.at[me], B.at[me], other, (tag, "d"))

        def relay():
            arrived((tag, "near"))
            pass_on(from_left, lo, right, "far")
            pass_on(from_right, hi, left, "far")
            pass_on(from_left, lo, other, "d")
            pass_on(from_right, hi, other, "d")

        def rest():
            arrived((tag, "next"))
            pass_on(from_left, hi, other, "d")
            pass_on(from_right, lo, other, "d")

        def far():
            arrived((tag, "far"))
            pass_on(across, lo, other, "d")
            pass_on(across, hi, other, "d")

        def end():
            arrived((tag, "d"))

        return start, relay, rest, far, end

    def scatter(S, Q, U, RL, F, tag):
        n = S.shape[2]
        lo, hi = slice(0, n // 2), slice(n // 2, n)
        right, left, other = at("x", 1), at("x", -1), at("c", 1)

        def hand_over(offset):
            b = near("x", offset)
            send(S.at[b, near("c", 1)], Q.at[b], other, (tag, "q", abs(offset)))

        def pair(offset, half):
            b = near("x", offset)
            return S[b, c, half, :].astype(F32) + Q[b, half, :].astype(F32)

        def first():
            arrived((tag, "q", 2))
            U[2, lo, :] = pair(2, lo).astype(BF16)
            send(U.at[2, lo], RL.at[lo], right, (tag, "far"))
            U[2, hi, :] = pair(2, hi).astype(BF16)
            send(U.at[2, hi], RL.at[hi], left, (tag, "far"))

        def second():
            arrived((tag, "q", 1))
            U[0, hi, :] = pair(1, hi).astype(BF16)
            send(U.at[0, hi], F.at[0, hi], right, (tag, "near"))
            U[1, lo, :] = pair(-1, lo).astype(BF16)
            send(U.at[1, lo], F.at[1, lo], left, (tag, "near"))

        def third():
            arrived((tag, "far"))
            U[0, lo, :] = (pair(1, lo) + RL[lo, :].astype(F32)).astype(BF16)
            send(U.at[0, lo], F.at[0, lo], right, (tag, "near"))
            U[1, hi, :] = (pair(-1, hi) + RL[hi, :].astype(F32)).astype(BF16)
            send(U.at[1, hi], F.at[1, hi], left, (tag, "near"))

        def total():
            arrived((tag, "q", 0))
            arrived((tag, "near"))
            return pair(0, slice(0, n)) + F[0].astype(F32) + F[1].astype(F32)

        return hand_over, first, second, third, total

    def norm(B, gain):
        def rows_of(i, carry):
            rows = pl.ds(pl.multiple_of(i * 128, 128), 128)
            squares = jnp.zeros((128, COLS), F32)
            for j in range(8):
                v = B[j, rows, :].astype(F32)
                squares = squares + v * v
            r = lax.rsqrt(jnp.sum(squares, axis=1, keepdims=True) * (1.0 / D) + EPS)
            for j in range(8):
                lanes = slice(COLS * j, COLS * j + COLS)
                N[rows, lanes] = (B[j, rows, :].astype(F32) * r * gain[:, lanes]).astype(BF16)
            return carry

        lax.fori_loop(0, 3, rows_of, 0)

    gather1, gather2 = gather(T, "g1"), gather(M, "g2")
    scatter1 = scatter(S1, Q1, U1, RL1, F1, "s1")
    scatters = (
        scatter(S2, Q2, U2, RL2, F2, "s2"), scatter(S3, Q3, U3, RL3, F3, "s3"),
    )

    def mixer():
        for s in MIX:
            finish(s)
        pooled_in = jnp.dot(N[...], PIN[...].reshape(D, 128), preferred_element_type=F32).astype(BF16)
        window = jnp.left_shift(jnp.int32(2), lax.rem(me, 4))
        later = lax.broadcasted_iota(jnp.int32, (LENGTH, LENGTH), 0)
        earlier = lax.broadcasted_iota(jnp.int32, (LENGTH, LENGTH), 1)
        inside = (earlier <= later) & (earlier > later - window)
        band = jnp.where(inside, 1.0, 0.0).astype(BF16)
        divisor = jnp.minimum(later + 1, window).astype(F32)
        grouped = []
        for s in range(ROWS // LENGTH):
            own = pooled_in[s * LENGTH : (s + 1) * LENGTH]
            sums = jnp.dot(band, own, preferred_element_type=F32)
            pooled = (sums / divisor - own.astype(F32)).astype(BF16)
            mapped = jnp.dot(pooled, group_weight[...], preferred_element_type=F32)
            grouped.append((mapped * channel_scale[...]).astype(BF16))
        GR[...] = jnp.concatenate(grouped, axis=0)
        mixer_out(2)

    def mixer_out(*offsets):
        for offset in offsets:
            b = near("x", offset)
            for core in (near("c", 1), c):
                piece = POUT[2 * b + core].reshape(COLS, 128)
                terms = lax.dot_general(GR[...], piece, (((1,), (1,)), ((), ())), preferred_element_type=F32)
                S1[b, core] = terms.astype(BF16)
            scatter1[0](offset)

    def middle():
        value = (T[me].astype(F32) + scatter1[4]()).astype(BF16)
        M[me] = value
        gather2[0]()
        MT[...] = jnp.transpose(value.astype(F32)).reshape(8, 32, ROWS)

    def silu_up(g, u):
        return g / (1.0 + jnp.exp(-g)) * u

    settled = set()

    def settle(i):
        for s in tile_streams(i):
            if s not in settled:
                finish(s)
                settled.add(s)

    def hidden(i):
        settle(i)
        piece = GU[:, :, :, 256 * i : 256 * i + 256].reshape(D, 256)
        acc = jnp.dot(N[...], piece, preferred_element_type=F32)
        h = silu_up(acc[:, :128], acc[:, 128:])
        HT[128 * i : 128 * i + 128, :] = jnp.transpose(h).astype(BF16)

    def hidden_tail():
        settle(5)
        acc = jnp.dot(N[...], GU[:, :, :, 1280:1408].reshape(D, 128), preferred_element_type=F32)
        h = silu_up(acc, pltpu.roll(acc, 64, 1))
        lane = lax.broadcasted_iota(jnp.int32, h.shape, 1)
        HT[640:768, :] = jnp.transpose(jnp.where(lane < 64, h, 0.0)).astype(BF16)

    def down(h, S, offset):
        if offset == 2:
            finish(DOWN[h])
        b = near("x", offset)
        rows = DOWN_ROWS[h][1]
        piece = DN[h][pl.ds(2 * b, 2)].reshape(16 * rows, HID)
        terms = jnp.dot(piece, HT[...], preferred_element_type=F32).astype(BF16)
        S[b] = terms.reshape(2, 8 * rows, ROWS)
        scatters[h][0](offset)

    def collect(h):
        first, rows = DOWN_ROWS[h]
        part_of = slice(first, first + rows)
        C[:, part_of] = scatters[h][4]().reshape(8, rows, ROWS) + MT[:, part_of]

    def last():
        closing = C[...].reshape(COLS, ROWS)
        own = jnp.sum(closing * closing, axis=0, keepdims=True)
        SQ[me] = jnp.broadcast_to(own, (8, ROWS))
        for peer in peers:
            send(SQ.at[me], SQ.at[me], peer, "squares")
        arrived("squares")
        squares = jnp.sum(SQ[...], axis=0)[0:1]
        scaled = C[...].reshape(COLS, ROWS) * lax.rsqrt(squares * (1.0 / D) + EPS)
        out[...] = (jnp.transpose(scaled) * final_gain[...]).astype(BF16)

    runs = {"norm1": lambda: norm(T, mixer_gain), "mixer": mixer, "mixer1": lambda: mixer_out(1, -1),
            "mixer2": lambda: mixer_out(0), "middle": middle, "norm2": lambda: norm(M, ffn_gain)}
    for s in range(len(STREAMS)):
        runs["w", s, 0, 4] = lambda s=s: spread(s)
        for phase in (1, 2):
            for k in range(1, 5):
                runs["w", s, phase, k] = lambda s=s, phase=phase, k=k: step(s, phase, k)
    for tag, parts in (("g1", gather1), ("g2", gather2), ("s1", scatter1), ("s2", scatters[0]), ("s3", scatters[1])):
        for i, part_run in enumerate(parts):
            runs[tag, i] = part_run
    runs["g2", 0] = lambda: None
    for i in range(5):
        runs["h", i] = lambda i=i: hidden(i)
    runs["h", 5] = hidden_tail
    for h, S in enumerate((S2, S3)):
        runs["c", h] = lambda h=h: collect(h)
        for offset in (2, 1, -1, 0):
            runs["d", h, offset] = lambda h=h, S=S, offset=offset: down(h, S, offset)
    runs["last"] = last
    for t, name in order(events()):
        next_event()
        runs[name]()
    for slot in range(SENDING):
        drain(slot)


def scatter_scratch(n, lanes):
    return [
        pltpu.VMEM((4, 2, n, lanes), BF16),
        pltpu.VMEM((4, n, lanes), BF16),
        pltpu.VMEM((3, n, lanes), BF16),
        pltpu.VMEM((n, lanes), BF16),
        pltpu.VMEM((2, n, lanes), BF16),
    ]


def local(
    tokens, mixer_gain, pool_input, group_weight, channel_scale, pool_output,
    ffn_gain, gate_weight, up_weight, down_weight, final_gain,
):
    vmem = pl.BlockSpec(memory_space=pltpu.VMEM)
    hbm = pl.BlockSpec(memory_space=pltpu.HBM)
    operands = (
        tokens, pool_input, pool_output.T, gate_weight, up_weight, down_weight.T, mixer_gain.reshape(1, D),
        group_weight.reshape(128, 128), channel_scale.reshape(1, 128), ffn_gain.reshape(1, D), final_gain.reshape(1, COLS),
    )
    return pl.pallas_call(
        kernel,
        out_shape=jax.ShapeDtypeStruct((ROWS, COLS), BF16),
        in_specs=[hbm] * 11,
        out_specs=vmem,
        scratch_shapes=[
            pltpu.VMEM((8, ROWS, COLS), BF16),
            pltpu.VMEM((8, ROWS, COLS), BF16),
            pltpu.VMEM((8, 8, 32, 128), BF16),
            pltpu.VMEM((8, 8, 32, 128), BF16),
            pltpu.VMEM((8, 8, 32, 1408), BF16),
            *(pltpu.VMEM((8, 8, rows, HID), BF16) for _, rows in DOWN_ROWS),
            pltpu.VMEM((ROWS, D), BF16),
            pltpu.VMEM((ROWS, 128), BF16),
            pltpu.VMEM((HID, ROWS), BF16),
            pltpu.VMEM((8, 32, ROWS), F32),
            pltpu.VMEM((8, 32, ROWS), F32),
            pltpu.VMEM((8, 8, ROWS), F32),
            pltpu.VMEM((32, 704), BF16),
            pltpu.VMEM((32, 704), BF16),
            pltpu.VMEM((32, 704), BF16),
            pltpu.VMEM((1, D), F32),
            pltpu.VMEM((128, 128), BF16),
            pltpu.VMEM((1, 128), F32),
            pltpu.VMEM((1, D), F32),
            pltpu.VMEM((1, COLS), F32),
            *scatter_scratch(ROWS, COLS),
            *(s for _, rows in DOWN_ROWS for s in scatter_scratch(8 * rows, ROWS)),
            pltpu.VMEM((3072, 128), BF16),
            pltpu.SemaphoreType.DMA((11,)),
            pltpu.SemaphoreType.DMA((SENDING,)),
            pltpu.SemaphoreType.DMA((ARRIVALS,)),
        ],
        compiler_params=pltpu.CompilerParams(
            collective_id=0, has_side_effects=True, vmem_limit_bytes=50 * 1024 * 1024
        ),
        name="layer",
    )(*(pltpu.with_memory_space_constraint(a, pltpu.HBM) for a in operands))


def solution(mesh):
    torus = Mesh(mesh.devices.reshape(8, 8, 4, 2), ("z", "y", "x", "c"))
    in_specs = (
        P(FS, TP),
        P(),
        P(FS, TP),
        P(TP, None, None),
        P(TP),
        P(TP, FS),
        P(),
        P(FS, TP),
        P(FS, TP),
        P(TP, FS),
        P(TP),
    )
    return jax.shard_map(local, mesh=torus, in_specs=in_specs, out_specs=P(FS, TP), check_vma=False)
```

```python
import jax
import jax.numpy as jnp
from jax import lax
from jax.experimental import pallas as pl
from jax.experimental.pallas import tpu as pltpu
from jax.sharding import Mesh
from jax.sharding import PartitionSpec as P

MESH = pl.DeviceIdType.MESH
F32 = jnp.float32
BF16 = jnp.bfloat16
D = 2048
ROWS = 384
COLS = 256
LENGTH = 128
FS = ("z", "y")
TP = ("x", "c")
EPS = 1e-06
SENDING = 32
ARRIVALS = 5 * 2 + 8 * 7 + 2 * 4 + 3 * 5 + 1

STREAMS = (
    ("PI", 0, 128, 16), ("PO", 0, 128, 16),
    ("G", 0, 512, 16),
    ("G", 512, 512, 16),
    ("G", 1024, 256, 16),
    ("G", 1280, 128, 16),
    ("T", 0, 128, 8),
    ("D0", 0, 320, 16),
    ("D1", 0, 320, 16),
)
DIRECT = (0, 1)
LINK = {1: (46.6e3, 2.9), -1: (46.6e3, 2.9), "x": (46.6e3, 2.7), "d": (500e3, 1.1)}
WINDOW = 3
EARLY = (2, 3)
FAR = 2.9
MIXER, CHAIN = -20, -20
MIX, GATES, TAIL, DOWN = (0, 1), (2, 3, 4, 5), 6, (7, 8)
DOWN_ROWS = ((0, 16), (16, 16))


def hops(stream, phase, sign):
    return 4 if phase == 2 or (stream % 2 == 0) == (sign > 0) else 3


def ahead(k):
    return (0,) if k == 1 else (k - 1, 1 - k)


def tile_streams(i):
    return [s for s in GATES if STREAMS[s][1] < 256 * i + 256 and STREAMS[s][1] + STREAMS[s][2] > 256 * i]


def events():
    plan = []

    def add(name, rank, needs=(), after=(), cost=0.1, sends=()):
        plan.append((name, rank, tuple(needs), tuple(after), cost, tuple(sends)))

    for s, (_, first, lanes, rows) in enumerate(STREAMS):
        piece = 2 * rows * lanes
        if s in DIRECT:
            add(("w", s, 0, 4), s - 20, sends=[(("w", s, 1, 4), sign, 8 * piece) for sign in (1, -1)])
        for phase in (1, 2):
            for k in range(1, 5):
                if phase == 1 and s in DIRECT:
                    continue
                needs = [("w", s, phase, k - 1)] if k > 1 else [("w", s, 1, 4)] if phase == 2 else []
                after = [("w", s - WINDOW, 2, 2)] if phase == 2 and k == 1 and s >= WINDOW and s not in EARLY else []
                after += [("w", s, 2, 1)] if (phase, k) == (2, 2) else []
                size = piece * (8 if phase == 2 else 1)
                cost = 0.05 if phase == 2 else 0.15
                size = size // 2 if (phase, k) == (2, 4) else size
                if s in EARLY and (phase, k) == (2, 1):
                    size = piece
                sends = [(("w", s, phase, k), sign, size) for sign in (1, -1) if k <= hops(s, phase, sign)]
                if s in EARLY and phase == 1:
                    sends += [(("w", s, 2, 1), sign, piece * len(ahead(k))) for sign in (1, -1)]
                add(("w", s, phase, k), s - 10, needs, after, cost, sends)

    def add_gather(tag, rank, first):
        half, over = ROWS * COLS, lambda *keys: [((tag, "d", k), "d", ROWS * COLS) for k in keys]
        sends = [((tag, "near"), "x", half), ((tag, "next"), "x", half), ((tag, "own"), "d", 2 * half)]
        add((tag, 0), rank, [], first, 0.1, sends)
        add((tag, 1), rank, [(tag, "near")], [(tag, 0)], 0.1, [((tag, "far"), "x", half)] + over(0, 1))
        add((tag, 2), rank, [(tag, "next")], [(tag, 1)], 0.1, over(2, 3))
        add((tag, 3), rank, [(tag, "far")], [(tag, 2)], 0.1, over(4, 5))
        add((tag, 4), rank, [(tag, "own")] + [(tag, "d", k) for k in range(6)], [(tag, 3)])

    def add_scatter(tag, rank, source, block):
        half = block // 2
        add((tag, 1), rank, [(tag, "q", 2)], [source], 0.1, [((tag, "far"), "x", half)])
        add((tag, 2), rank + 0, [(tag, "q", 1), (tag, "q", -1)], [(tag, 1)] + (["mixer1"] if tag == "s1" else []), 0.1, [((tag, "one"), "x", half)])
        add((tag, 3), rank, [(tag, "far")], [(tag, 2)], 0.1, [((tag, "two"), "x", half)])

    def whole(tag):
        return [(tag, "two"), (tag, "one"), (tag, "q", 0)]

    block1 = 2 * ROWS * COLS
    add_gather("g1", -30, [])
    add("norm1", 0, [], [("g1", 4)], 0.7)
    add("mixer", MIXER, [("w", s, 2, 4) for s in MIX], ["norm1"], 2.0, [(("s1", "q", 2), "d", block1)])
    add("mixer1", MIXER, [], ["mixer"], 0.9, [(("s1", "q", o), "d", block1) for o in (1, -1)])
    add("mixer2", MIXER, [], ["mixer1"], 0.5, [(("s1", "q", 0), "d", block1)])
    add_scatter("s1", CHAIN, "mixer", block1)
    add_gather("g2", CHAIN, ["middle"])
    add("middle", CHAIN, whole("s1"), [("s1", 3), "mixer2"], 0.4)
    add("norm2", 0, [], [("g2", 4)], 0.7)
    for i in range(6):
        add(("h", i), 0, [("w", s, 2, 4) for s in tile_streams(i)], [("h", i - 1)] if i else ["norm2"], 1.06)
    for h, (_, rows) in enumerate(DOWN_ROWS):
        tag, before, block2 = f"s{2 + h}", ("h", 5), 2 * ROWS * 8 * rows
        for offset in (2, 1, -1, 0):
            name = ("d", h, offset)
            add(name, h, [("w", TAIL, 2, 4), ("w", DOWN[h], 2, 4)], [before], 0.17 + 0.0125 * rows, [((tag, "q", offset), "d", block2)])
            before = name
        add_scatter(tag, h - 4, ("d", h, 2), block2)
        add(("c", h), h - 4, whole(tag), [(tag, 3)], 0.025 * rows)
    add("last", 9, [], [("c", h) for h in range(len(DOWN))], 4.0)
    return plan


def order(plan, margin=0.15):
    now, free, arrival, done, left, result = 0.0, {}, {}, set(), list(plan), []
    while left:
        best = None
        for e in left:
            name, rank, needs, after, cost, sends = e
            if any(k not in arrival for k in needs) or any(k not in done for k in after):
                continue
            key = (max([now] + [arrival[k] + margin for k in needs]), rank)
            if best is None or key < best[0]:
                best = (key, e)
        (ready, _), e = best
        name, rank, needs, after, cost, sends = e
        now = ready + cost
        done.add(name)
        for key, link, size in sends:
            rate, delay = LINK[link]
            free[link] = max(free.get(link, 0.0), now) + size / rate
            arrival[key] = max(arrival.get(key, 0.0), free[link] + delay + (FAR if name[:1] == ("w",) and name[2] == 0 else 0.0))
        left.remove(e)
        result.append((ready, name))
    return result


def kernel(
    tok, pool_in, pool_out, gate, up, down_t, mixer_gain_in, group_weight_in, channel_scale_in, ffn_gain_in,
    final_gain_in, out,
    T, M, PIN, POUT, GU, DN0, DN1, DTA, DTB, N, GR, HT, HTT, MT, C, SQ,
    gate_own, up_own, down_own, mixer_gain, group_weight, channel_scale, ffn_gain, final_gain,
    S1, Q1, U1, RL1, F1, S2, Q2, U2, RL2, F2, S3, Q3, U3, RL3, F3, W,
    local_sem, send_sem, recv_sem,
):
    z, y, x, c = (lax.axis_index(n) for n in ("z", "y", "x", "c"))
    me = 2 * x + c
    DN = (DN0, DN1)
    place = {"z": z, "y": y, "x": x, "c": c}
    size = {"z": 8, "y": 8, "x": 4, "c": 2}

    def near(axis, offset):
        return lax.rem(place[axis] + (offset + size[axis]), size[axis])

    def at(axis, offset):
        return {axis: near(axis, offset)}

    barrier = pltpu.get_barrier_semaphore()
    friends = [at(axis, o) for o in (4, 3, -3, 2, -2, 1, -1) for axis in ("z", "y")]
    peers = [{"x": near("x", dx), "c": near("c", dc)} for dx in range(4) for dc in range(2) if (dx, dc) != (0, 0)]
    for friend in friends + peers:
        pl.semaphore_signal(barrier, inc=1, device_id=friend, device_id_type=MESH)
    local_copies = [
        (gate, gate_own), (up, up_own), (down_t, down_own), (pool_in, PIN.at[z, y]), (pool_out, POUT.at[z, y]),
        (tok, T.at[me]), (mixer_gain_in, mixer_gain), (group_weight_in, group_weight),
        (channel_scale_in, channel_scale), (ffn_gain_in, ffn_gain), (final_gain_in, final_gain),
    ]
    local_copies = [pltpu.make_async_copy(a, b, local_sem.at[i]) for i, (a, b) in enumerate(local_copies)]
    for copy in local_copies:
        copy.start()

    for copy in local_copies:
        copy.wait()
    for i in range(5):
        GU[z, y, :, 256 * i : 256 * i + 128] = gate_own[:, 128 * i : 128 * i + 128]
        GU[z, y, :, 256 * i + 128 : 256 * i + 256] = up_own[:, 128 * i : 128 * i + 128]
    GU[z, y, :, 1280:1408] = jnp.concatenate([gate_own[:, 640:], up_own[:, 640:]], axis=1)
    for h, (first, rows) in enumerate(DOWN_ROWS):
        DN[h][z, y] = down_own[first : first + rows, :640]
    tails = jnp.concatenate([down_own[:16, 640:], down_own[16:, 640:]], axis=1)
    DTA[z, y] = tails[:8]
    DTB[z, y] = tails[8:]
    pl.semaphore_wait(barrier, len(friends) + len(peers))

    leaving, groups, turn = [0] * SENDING, {}, [0]

    def drain(slot):
        if leaving[slot]:
            ref = W.at[pl.ds(0, leaving[slot] // 256)]
            pltpu.make_async_copy(ref, ref, send_sem.at[slot]).wait()
            leaving[slot] = 0

    def next_event():
        turn[0] = (turn[0] + 1) % SENDING
        drain(turn[0])

    def send(src, dst, device, group):
        slot, size = groups.setdefault(group, (len(groups), 0))
        bytes_of = dst.dtype.itemsize
        for n in dst.shape:
            bytes_of *= n
        groups[group] = (slot, size + bytes_of)
        leaving[turn[0]] += bytes_of
        pltpu.make_async_remote_copy(
            src_ref=src, dst_ref=dst, send_sem=send_sem.at[turn[0]], recv_sem=recv_sem.at[slot],
            device_id=device, device_id_type=MESH,
        ).start()

    def arrived(group):
        slot, size = groups[group]
        ref = W.at[pl.ds(0, size // 256)]
        pltpu.make_async_copy(ref, ref, recv_sem.at[slot]).wait()

    def part(s, route, zi, yi):
        name, first, lanes, rows = STREAMS[s]
        if name[0] == "D":
            h = int(name[1])
            cut = 384 if h else 256
            ref, tail = DN[h], (slice(None), pl.ds(cut, 640 - cut) if route else pl.ds(0, cut))
        elif name == "T":
            ref, tail = (DTA, DTB)[route], (slice(None), slice(None))
        else:
            ref = {"PI": PIN, "PO": POUT, "G": GU}[name]
            tail = (pl.ds(16 * route, 16), pl.ds(first, lanes))
        return ref.at[(zi, yi) + tail]

    def slab(s, route, phase, origin, whole=slice(None)):
        if phase == 1:
            return part(s, route, z, origin) if route == 0 else part(s, route, origin, y)
        return part(s, route, origin, whole) if route == 0 else part(s, route, whole, origin)

    def spread(s):
        for route in range(2):
            axis = "yz"[route]
            ref = slab(s, route, 1, place[axis])
            for offset in (1, -1, 2, -2, 3, -3, 4):
                send(ref, ref, at(axis, offset), ("w", s, 1, 4))

    def send_ahead(s, offsets):
        for route in range(2):
            for sign in (1, -1):
                for offset in offsets:
                    ref = slab(s, route, 1, near("yz"[route], offset))
                    send(ref, ref, at("zy"[route], sign), ("w", s, 2, 1))

    def step(s, phase, k):
        if k > 1:
            arrived(("w", s, phase, k - 1))
        elif phase == 2:
            arrived(("w", s, 1, 4))
        if s in EARLY and (phase, k) == (2, 1):
            send_ahead(s, (4,))
            return
        for route in range(2):
            axis = "y" if (route == 0) == (phase == 1) else "z"
            for sign in (1, -1):
                if k <= hops(s, phase, sign):
                    pieces = slice(None) if (phase, k) != (2, 4) else slice(0, 4) if sign > 0 else slice(4, 8)
                    ref = slab(s, route, phase, near(axis, -sign * (k - 1)), pieces)
                    send(ref, ref, at(axis, sign), ("w", s, phase, k))
        if s in EARLY and phase == 1:
            send_ahead(s, ahead(k))

    def finish(s):
        arrived(("w", s, 2, 4))

    def gather(B, tag):
        lo, hi = slice(0, ROWS // 2), slice(ROWS // 2, ROWS)
        right, left, other = at("x", 1), at("x", -1), at("c", 1)
        from_left, from_right, across = (2 * near("x", o) + c for o in (-1, 1, 2))

        def pass_on(block, half, device, group):
            ref = B.at[block, half]
            send(ref, ref, device, (tag, group))

        def start():
            pass_on(me, lo, right, "near")
            pass_on(me, hi, left, "near")
            pass_on(me, hi, right, "next")
            pass_on(me, lo, left, "next")
            send(B.at[me], B.at[me], other, (tag, "d"))

        def relay():
            arrived((tag, "near"))
            pass_on(from_left, lo, right, "far")
            pass_on(from_right, hi, left, "far")
            pass_on(from_left, lo, other, "d")
            pass_on(from_right, hi, other, "d")

        def rest():
            arrived((tag, "next"))
            pass_on(from_left, hi, other, "d")
            pass_on(from_right, lo, other, "d")

        def far():
            arrived((tag, "far"))
            pass_on(across, lo, other, "d")
            pass_on(across, hi, other, "d")

        def end():
            arrived((tag, "d"))

        return start, relay, rest, far, end

    def scatter(S, Q, U, RL, F, tag):
        n = S.shape[2]
        lo, hi = slice(0, n // 2), slice(n // 2, n)
        right, left, other = at("x", 1), at("x", -1), at("c", 1)

        def hand_over(offset):
            b = near("x", offset)
            send(S.at[b, near("c", 1)], Q.at[b], other, (tag, "q", abs(offset)))

        def pair(offset, half):
            b = near("x", offset)
            return S[b, c, half, :].astype(F32) + Q[b, half, :].astype(F32)

        def first():
            arrived((tag, "q", 2))
            U[2, lo, :] = pair(2, lo).astype(BF16)
            send(U.at[2, lo], RL.at[lo], right, (tag, "far"))
            U[2, hi, :] = pair(2, hi).astype(BF16)
            send(U.at[2, hi], RL.at[hi], left, (tag, "far"))

        def second():
            arrived((tag, "q", 1))
            U[0, hi, :] = pair(1, hi).astype(BF16)
            send(U.at[0, hi], F.at[0, hi], right, (tag, "near"))
            U[1, lo, :] = pair(-1, lo).astype(BF16)
            send(U.at[1, lo], F.at[1, lo], left, (tag, "near"))

        def third():
            arrived((tag, "far"))
            U[0, lo, :] = (pair(1, lo) + RL[lo, :].astype(F32)).astype(BF16)
            send(U.at[0, lo], F.at[0, lo], right, (tag, "near"))
            U[1, hi, :] = (pair(-1, hi) + RL[hi, :].astype(F32)).astype(BF16)
            send(U.at[1, hi], F.at[1, hi], left, (tag, "near"))

        def total():
            arrived((tag, "q", 0))
            arrived((tag, "near"))
            return pair(0, slice(0, n)) + F[0].astype(F32) + F[1].astype(F32)

        return hand_over, first, second, third, total

    def norm(B, gain):
        def rows_of(i, carry):
            rows = pl.ds(pl.multiple_of(i * 128, 128), 128)
            squares = jnp.zeros((128, COLS), F32)
            for j in range(8):
                v = B[j, rows, :].astype(F32)
                squares = squares + v * v
            r = lax.rsqrt(jnp.sum(squares, axis=1, keepdims=True) * (1.0 / D) + EPS)
            for j in range(8):
                lanes = slice(COLS * j, COLS * j + COLS)
                N[rows, lanes] = (B[j, rows, :].astype(F32) * r * gain[:, lanes]).astype(BF16)
            return carry

        lax.fori_loop(0, 3, rows_of, 0)

    gather1, gather2 = gather(T, "g1"), gather(M, "g2")
    scatter1 = scatter(S1, Q1, U1, RL1, F1, "s1")
    scatters = (
        scatter(S2, Q2, U2, RL2, F2, "s2"), scatter(S3, Q3, U3, RL3, F3, "s3"),
    )

    def mixer():
        for s in MIX:
            finish(s)
        pooled_in = jnp.dot(N[...], PIN[...].reshape(D, 128), preferred_element_type=F32).astype(BF16)
        window = jnp.left_shift(jnp.int32(2), lax.rem(me, 4))
        later = lax.broadcasted_iota(jnp.int32, (LENGTH, LENGTH), 0)
        earlier = lax.broadcasted_iota(jnp.int32, (LENGTH, LENGTH), 1)
        inside = (earlier <= later) & (earlier > later - window)
        band = jnp.where(inside, 1.0, 0.0).astype(BF16)
        divisor = jnp.minimum(later + 1, window).astype(F32)
        grouped = []
        for s in range(ROWS // LENGTH):
            own = pooled_in[s * LENGTH : (s + 1) * LENGTH]
            sums = jnp.dot(band, own, preferred_element_type=F32)
            pooled = (sums / divisor - own.astype(F32)).astype(BF16)
            mapped = jnp.dot(pooled, group_weight[...], preferred_element_type=F32)
            grouped.append((mapped * channel_scale[...]).astype(BF16))
        GR[...] = jnp.concatenate(grouped, axis=0)
        mixer_out(2)

    def mixer_out(*offsets):
        for offset in offsets:
            b = near("x", offset)
            for core in (near("c", 1), c):
                piece = POUT[2 * b + core].reshape(COLS, 128)
                terms = lax.dot_general(GR[...], piece, (((1,), (1,)), ((), ())), preferred_element_type=F32)
                S1[b, core] = terms.astype(BF16)
            scatter1[0](offset)

    def middle():
        value = (T[me].astype(F32) + scatter1[4]()).astype(BF16)
        M[me] = value
        gather2[0]()
        MT[...] = jnp.transpose(value.astype(F32)).reshape(8, 32, ROWS)

    def silu_up(g, u):
        return g / (1.0 + jnp.exp(-g)) * u

    settled = set()

    def settle(i):
        for s in tile_streams(i):
            if s not in settled:
                finish(s)
                settled.add(s)

    def hidden(i):
        settle(i)
        piece = GU[:, :, :, 256 * i : 256 * i + 256].reshape(D, 256)
        acc = jnp.dot(N[...], piece, preferred_element_type=F32)
        h = silu_up(acc[:, :128], acc[:, 128:])
        HT[128 * i : 128 * i + 128, :] = jnp.transpose(h).astype(BF16)

    def hidden_tail():
        settle(5)
        acc = jnp.dot(N[...], GU[:, :, :, 1280:1408].reshape(D, 128), preferred_element_type=F32)
        h = silu_up(acc, pltpu.roll(acc, 64, 1))
        lane = lax.broadcasted_iota(jnp.int32, h.shape, 1)
        h = jnp.where(lane < 64, h, 0.0)
        HTT[0] = jnp.transpose(h).astype(BF16)
        HTT[1] = jnp.transpose(pltpu.roll(h, 64, 1)).astype(BF16)

    def down(h, S, offset):
        if offset == 2:
            if h == 0:
                finish(TAIL)
            finish(DOWN[h])
        b = near("x", offset)
        rows = DOWN_ROWS[h][1]
        both = pl.ds(2 * b, 2)
        end = jnp.concatenate([DTA[both], DTB[both]], axis=2).reshape(16 * rows, 128)
        piece = jnp.concatenate([DN[h][both].reshape(16 * rows, 640), end], axis=1)
        right = jnp.concatenate([HT[...], HTT[h]], axis=0)
        terms = jnp.dot(piece, right, preferred_element_type=F32).astype(BF16)
        S[b] = terms.reshape(2, 8 * rows, ROWS)
        scatters[h][0](offset)

    def collect(h):
        first, rows = DOWN_ROWS[h]
        part_of = slice(first, first + rows)
        C[:, part_of] = scatters[h][4]().reshape(8, rows, ROWS) + MT[:, part_of]

    def last():
        closing = C[...].reshape(COLS, ROWS)
        own = jnp.sum(closing * closing, axis=0, keepdims=True)
        SQ[me] = jnp.broadcast_to(own, (8, ROWS))
        for peer in peers:
            send(SQ.at[me], SQ.at[me], peer, "squares")
        arrived("squares")
        squares = jnp.sum(SQ[...], axis=0)[0:1]
        scaled = C[...].reshape(COLS, ROWS) * lax.rsqrt(squares * (1.0 / D) + EPS)
        out[...] = (jnp.transpose(scaled) * final_gain[...]).astype(BF16)

    runs = {"norm1": lambda: norm(T, mixer_gain), "mixer": mixer, "mixer1": lambda: mixer_out(1, -1),
            "mixer2": lambda: mixer_out(0), "middle": middle, "norm2": lambda: norm(M, ffn_gain)}
    for s in range(len(STREAMS)):
        runs["w", s, 0, 4] = lambda s=s: spread(s)
        for phase in (1, 2):
            for k in range(1, 5):
                runs["w", s, phase, k] = lambda s=s, phase=phase, k=k: step(s, phase, k)
    for tag, parts in (("g1", gather1), ("g2", gather2), ("s1", scatter1), ("s2", scatters[0]), ("s3", scatters[1])):
        for i, part_run in enumerate(parts):
            runs[tag, i] = part_run
    runs["g2", 0] = lambda: None
    for i in range(5):
        runs["h", i] = lambda i=i: hidden(i)
    runs["h", 5] = hidden_tail
    for h, S in enumerate((S2, S3)):
        runs["c", h] = lambda h=h: collect(h)
        for offset in (2, 1, -1, 0):
            runs["d", h, offset] = lambda h=h, S=S, offset=offset: down(h, S, offset)
    runs["last"] = last
    for t, name in order(events()):
        next_event()
        runs[name]()
    for slot in range(SENDING):
        drain(slot)


def scatter_scratch(n, lanes):
    return [
        pltpu.VMEM((4, 2, n, lanes), BF16),
        pltpu.VMEM((4, n, lanes), BF16),
        pltpu.VMEM((3, n, lanes), BF16),
        pltpu.VMEM((n, lanes), BF16),
        pltpu.VMEM((2, n, lanes), BF16),
    ]


def local(
    tokens, mixer_gain, pool_input, group_weight, channel_scale, pool_output,
    ffn_gain, gate_weight, up_weight, down_weight, final_gain,
):
    vmem = pl.BlockSpec(memory_space=pltpu.VMEM)
    hbm = pl.BlockSpec(memory_space=pltpu.HBM)
    operands = (
        tokens, pool_input, pool_output.T, gate_weight, up_weight, down_weight.T, mixer_gain.reshape(1, D),
        group_weight.reshape(128, 128), channel_scale.reshape(1, 128), ffn_gain.reshape(1, D), final_gain.reshape(1, COLS),
    )
    return pl.pallas_call(
        kernel,
        out_shape=jax.ShapeDtypeStruct((ROWS, COLS), BF16),
        in_specs=[hbm] * 11,
        out_specs=vmem,
        scratch_shapes=[
            pltpu.VMEM((8, ROWS, COLS), BF16),
            pltpu.VMEM((8, ROWS, COLS), BF16),
            pltpu.VMEM((8, 8, 32, 128), BF16),
            pltpu.VMEM((8, 8, 32, 128), BF16),
            pltpu.VMEM((8, 8, 32, 1408), BF16),
            *(pltpu.VMEM((8, 8, rows, 640), BF16) for _, rows in DOWN_ROWS),
            pltpu.VMEM((8, 8, 8, 128), BF16),
            pltpu.VMEM((8, 8, 8, 128), BF16),
            pltpu.VMEM((ROWS, D), BF16),
            pltpu.VMEM((ROWS, 128), BF16),
            pltpu.VMEM((640, ROWS), BF16),
            pltpu.VMEM((2, 128, ROWS), BF16),
            pltpu.VMEM((8, 32, ROWS), F32),
            pltpu.VMEM((8, 32, ROWS), F32),
            pltpu.VMEM((8, 8, ROWS), F32),
            pltpu.VMEM((32, 704), BF16),
            pltpu.VMEM((32, 704), BF16),
            pltpu.VMEM((32, 704), BF16),
            pltpu.VMEM((1, D), F32),
            pltpu.VMEM((128, 128), BF16),
            pltpu.VMEM((1, 128), F32),
            pltpu.VMEM((1, D), F32),
            pltpu.VMEM((1, COLS), F32),
            *scatter_scratch(ROWS, COLS),
            *(s for _, rows in DOWN_ROWS for s in scatter_scratch(8 * rows, ROWS)),
            pltpu.VMEM((3072, 128), BF16),
            pltpu.SemaphoreType.DMA((11,)),
            pltpu.SemaphoreType.DMA((SENDING,)),
            pltpu.SemaphoreType.DMA((ARRIVALS,)),
        ],
        compiler_params=pltpu.CompilerParams(
            collective_id=0, has_side_effects=True, vmem_limit_bytes=50 * 1024 * 1024
        ),
        name="layer",
    )(*(pltpu.with_memory_space_constraint(a, pltpu.HBM) for a in operands))


def solution(mesh):
    torus = Mesh(mesh.devices.reshape(8, 8, 4, 2), ("z", "y", "x", "c"))
    in_specs = (
        P(FS, TP),
        P(),
        P(FS, TP),
        P(TP, None, None),
        P(TP),
        P(TP, FS),
        P(),
        P(FS, TP),
        P(FS, TP),
        P(TP, FS),
        P(TP),
    )
    return jax.shard_map(local, mesh=torus, in_specs=in_specs, out_specs=P(FS, TP), check_vma=False)
```

```python
import jax
import jax.numpy as jnp
from jax import lax
from jax.experimental import pallas as pl
from jax.experimental.pallas import tpu as pltpu
from jax.sharding import Mesh
from jax.sharding import PartitionSpec as P

MESH = pl.DeviceIdType.MESH
F32 = jnp.float32
BF16 = jnp.bfloat16
D = 2048
ROWS = 384
COLS = 256
LENGTH = 128
FS = ("z", "y")
TP = ("x", "c")
EPS = 1e-06
SENDING = 32
ARRIVALS = 5 * 2 + 8 * 7 + 2 * 4 + 3 * 5 + 1

STREAMS = (
    ("PI", 0, 128, 16), ("PO", 0, 128, 16),
    ("G", 0, 512, 16),
    ("G", 512, 512, 16),
    ("G", 1024, 256, 16),
    ("G", 1280, 128, 16),
    ("T", 0, 128, 8),
    ("D0", 0, 320, 16),
    ("D1", 0, 320, 16),
)
DIRECT = (0, 1)
LINK = {1: (46.6e3, 2.9), -1: (46.6e3, 2.9), "x": (46.6e3, 2.7), "d": (500e3, 1.1)}
WINDOW = 3
EARLY = (2, 3)
FAR = 2.9
MIXER, CHAIN = -20, -20
MIX, GATES, TAIL, DOWN = (0, 1), (2, 3, 4, 5), 6, (7, 8)
DOWN_ROWS = ((0, 16), (16, 16))


def hops(stream, phase, sign):
    return 4 if phase == 2 or (stream % 2 == 0) == (sign > 0) else 3


def ahead(k):
    return (0,) if k == 1 else (k - 1, 1 - k)


def tile_streams(i):
    return [s for s in GATES if STREAMS[s][1] < 256 * i + 256 and STREAMS[s][1] + STREAMS[s][2] > 256 * i]


def events():
    plan = []

    def add(name, rank, needs=(), after=(), cost=0.1, sends=()):
        plan.append((name, rank, tuple(needs), tuple(after), cost, tuple(sends)))

    for s, (_, first, lanes, rows) in enumerate(STREAMS):
        piece = 2 * rows * lanes
        if s in DIRECT:
            add(("w", s, 0, 4), s - 20, sends=[(("w", s, 1, 4), sign, 8 * piece) for sign in (1, -1)])
        for phase in (1, 2):
            for k in range(1, 5):
                if phase == 1 and s in DIRECT:
                    continue
                needs = [("w", s, phase, k - 1)] if k > 1 else [("w", s, 1, 4)] if phase == 2 else []
                after = [("w", s - WINDOW, 2, 2)] if phase == 2 and k == 1 and s >= WINDOW and s not in EARLY else []
                after += [("w", s, 2, 1)] if (phase, k) == (2, 2) else []
                size = piece * (8 if phase == 2 else 1)
                cost = 0.05 if phase == 2 else 0.15
                size = size // 2 if (phase, k) == (2, 4) else size
                if s in EARLY and (phase, k) == (2, 1):
                    size = piece
                sends = [(("w", s, phase, k), sign, size) for sign in (1, -1) if k <= hops(s, phase, sign)]
                if s in EARLY and phase == 1:
                    sends += [(("w", s, 2, 1), sign, piece * len(ahead(k))) for sign in (1, -1)]
                add(("w", s, phase, k), s - 10, needs, after, cost, sends)

    def add_gather(tag, rank, first):
        half, over = ROWS * COLS, lambda *keys: [((tag, "d", k), "d", ROWS * COLS) for k in keys]
        sends = [((tag, "near"), "x", half), ((tag, "next"), "x", half), ((tag, "own"), "d", 2 * half)]
        add((tag, 0), rank, [], first, 0.1, sends)
        add((tag, 1), rank, [(tag, "near")], [(tag, 0)], 0.1, [((tag, "far"), "x", half)] + over(0, 1))
        add((tag, 2), rank, [(tag, "next")], [(tag, 1)], 0.1, over(2, 3))
        add((tag, 3), rank, [(tag, "far")], [(tag, 2)], 0.1, over(4, 5))
        add((tag, 4), rank, [(tag, "own")] + [(tag, "d", k) for k in range(6)], [(tag, 3)])

    def add_scatter(tag, rank, source, block):
        half = block // 2
        add((tag, 1), rank, [(tag, "q", 2)], [source], 0.1, [((tag, "far"), "x", half)])
        add((tag, 2), rank + 0, [(tag, "q", 1), (tag, "q", -1)], [(tag, 1)] + (["mixer1"] if tag == "s1" else []), 0.1, [((tag, "one"), "x", half)])
        add((tag, 3), rank, [(tag, "far")], [(tag, 2)], 0.1, [((tag, "two"), "x", half)])

    def whole(tag):
        return [(tag, "two"), (tag, "one"), (tag, "q", 0)]

    block1 = 2 * ROWS * COLS
    add_gather("g1", -30, [])
    add("norm1", 0, [], [("g1", 4)], 0.7)
    add("mixer", MIXER, [("w", MIX[0], 2, 4)], ["norm1"], 1.2)
    add("mixer0", MIXER, [("w", MIX[1], 2, 4)], ["mixer"], 0.8, [(("s1", "q", 2), "d", block1)])
    add("mixer1", MIXER, [], ["mixer0"], 0.9, [(("s1", "q", o), "d", block1) for o in (1, -1)])
    add("mixer2", MIXER, [], ["mixer1"], 0.5, [(("s1", "q", 0), "d", block1)])
    add_scatter("s1", CHAIN, "mixer0", block1)
    add_gather("g2", CHAIN, ["middle"])
    add("middle", CHAIN, whole("s1"), [("s1", 3), "mixer2"], 0.4)
    add("norm2", 0, [], [("g2", 4)], 0.7)
    for i in range(6):
        add(("h", i), 0, [("w", s, 2, 4) for s in tile_streams(i)], [("h", i - 1)] if i else ["norm2"], 1.06)
    for h, (_, rows) in enumerate(DOWN_ROWS):
        tag, before, block2 = f"s{2 + h}", ("h", 5), 2 * ROWS * 8 * rows
        for offset in (2, 1, -1, 0):
            name = ("d", h, offset)
            add(name, h, [("w", TAIL, 2, 4), ("w", DOWN[h], 2, 4)], [before], 0.17 + 0.0125 * rows, [((tag, "q", offset), "d", block2)])
            before = name
        add_scatter(tag, h - 4, ("d", h, 2), block2)
        add(("c", h), h - 4, whole(tag), [(tag, 3)], 0.025 * rows)
    add("last", 9, [], [("c", h) for h in range(len(DOWN))], 4.0)
    return plan


def order(plan, margin=0.15):
    now, free, arrival, done, left, result = 0.0, {}, {}, set(), list(plan), []
    while left:
        best = None
        for e in left:
            name, rank, needs, after, cost, sends = e
            if any(k not in arrival for k in needs) or any(k not in done for k in after):
                continue
            key = (max([now] + [arrival[k] + margin for k in needs]), rank)
            if best is None or key < best[0]:
                best = (key, e)
        (ready, _), e = best
        name, rank, needs, after, cost, sends = e
        now = ready + cost
        done.add(name)
        for key, link, size in sends:
            rate, delay = LINK[link]
            free[link] = max(free.get(link, 0.0), now) + size / rate
            arrival[key] = max(arrival.get(key, 0.0), free[link] + delay + (FAR if name[:1] == ("w",) and name[2] == 0 else 0.0))
        left.remove(e)
        result.append((ready, name))
    return result


def kernel(
    tok, pool_in, pool_out, gate, up, down_t, mixer_gain_in, group_weight_in, channel_scale_in, ffn_gain_in,
    final_gain_in, out,
    T, M, PIN, POUT, GU, DN0, DN1, DTA, DTB, N, GR, HT, HTT, MT, C, SQ,
    gate_own, up_own, down_own, mixer_gain, group_weight, channel_scale, ffn_gain, final_gain,
    S1, Q1, U1, RL1, F1, S2, Q2, U2, RL2, F2, S3, Q3, U3, RL3, F3, W,
    local_sem, send_sem, recv_sem,
):
    z, y, x, c = (lax.axis_index(n) for n in ("z", "y", "x", "c"))
    me = 2 * x + c
    DN = (DN0, DN1)
    place = {"z": z, "y": y, "x": x, "c": c}
    size = {"z": 8, "y": 8, "x": 4, "c": 2}

    def near(axis, offset):
        return lax.rem(place[axis] + (offset + size[axis]), size[axis])

    def at(axis, offset):
        return {axis: near(axis, offset)}

    barrier = pltpu.get_barrier_semaphore()
    friends = [at(axis, o) for o in (4, 3, -3, 2, -2, 1, -1) for axis in ("z", "y")]
    peers = [{"x": near("x", dx), "c": near("c", dc)} for dx in range(4) for dc in range(2) if (dx, dc) != (0, 0)]
    for friend in friends + peers:
        pl.semaphore_signal(barrier, inc=1, device_id=friend, device_id_type=MESH)
    local_copies = [
        (gate, gate_own), (up, up_own), (down_t, down_own), (pool_in, PIN.at[z, y]), (pool_out, POUT.at[z, y]),
        (tok, T.at[me]), (mixer_gain_in, mixer_gain), (group_weight_in, group_weight),
        (channel_scale_in, channel_scale), (ffn_gain_in, ffn_gain), (final_gain_in, final_gain),
    ]
    local_copies = [pltpu.make_async_copy(a, b, local_sem.at[i]) for i, (a, b) in enumerate(local_copies)]
    for copy in local_copies:
        copy.start()

    for copy in local_copies:
        copy.wait()
    for i in range(5):
        GU[z, y, :, 256 * i : 256 * i + 128] = gate_own[:, 128 * i : 128 * i + 128]
        GU[z, y, :, 256 * i + 128 : 256 * i + 256] = up_own[:, 128 * i : 128 * i + 128]
    GU[z, y, :, 1280:1408] = jnp.concatenate([gate_own[:, 640:], up_own[:, 640:]], axis=1)
    for h, (first, rows) in enumerate(DOWN_ROWS):
        DN[h][z, y] = down_own[first : first + rows, :640]
    tails = jnp.concatenate([down_own[:16, 640:], down_own[16:, 640:]], axis=1)
    DTA[z, y] = tails[:8]
    DTB[z, y] = tails[8:]
    pl.semaphore_wait(barrier, len(friends) + len(peers))

    leaving, groups, turn = [0] * SENDING, {}, [0]

    def drain(slot):
        if leaving[slot]:
            ref = W.at[pl.ds(0, leaving[slot] // 256)]
            pltpu.make_async_copy(ref, ref, send_sem.at[slot]).wait()
            leaving[slot] = 0

    def next_event():
        turn[0] = (turn[0] + 1) % SENDING
        drain(turn[0])

    def send(src, dst, device, group):
        slot, size = groups.setdefault(group, (len(groups), 0))
        bytes_of = dst.dtype.itemsize
        for n in dst.shape:
            bytes_of *= n
        groups[group] = (slot, size + bytes_of)
        leaving[turn[0]] += bytes_of
        pltpu.make_async_remote_copy(
            src_ref=src, dst_ref=dst, send_sem=send_sem.at[turn[0]], recv_sem=recv_sem.at[slot],
            device_id=device, device_id_type=MESH,
        ).start()

    def arrived(group):
        slot, size = groups[group]
        ref = W.at[pl.ds(0, size // 256)]
        pltpu.make_async_copy(ref, ref, recv_sem.at[slot]).wait()

    def part(s, route, zi, yi):
        name, first, lanes, rows = STREAMS[s]
        if name[0] == "D":
            h = int(name[1])
            cut = 384 if h else 256
            ref, tail = DN[h], (slice(None), pl.ds(cut, 640 - cut) if route else pl.ds(0, cut))
        elif name == "T":
            ref, tail = (DTA, DTB)[route], (slice(None), slice(None))
        else:
            ref = {"PI": PIN, "PO": POUT, "G": GU}[name]
            tail = (pl.ds(16 * route, 16), pl.ds(first, lanes))
        return ref.at[(zi, yi) + tail]

    def slab(s, route, phase, origin, whole=slice(None)):
        if phase == 1:
            return part(s, route, z, origin) if route == 0 else part(s, route, origin, y)
        return part(s, route, origin, whole) if route == 0 else part(s, route, whole, origin)

    def spread(s):
        for route in range(2):
            axis = "yz"[route]
            ref = slab(s, route, 1, place[axis])
            for offset in (1, -1, 2, -2, 3, -3, 4):
                send(ref, ref, at(axis, offset), ("w", s, 1, 4))

    def send_ahead(s, offsets):
        for route in range(2):
            for sign in (1, -1):
                for offset in offsets:
                    ref = slab(s, route, 1, near("yz"[route], offset))
                    send(ref, ref, at("zy"[route], sign), ("w", s, 2, 1))

    def step(s, phase, k):
        if k > 1:
            arrived(("w", s, phase, k - 1))
        elif phase == 2:
            arrived(("w", s, 1, 4))
        if s in EARLY and (phase, k) == (2, 1):
            send_ahead(s, (4,))
            return
        for route in range(2):
            axis = "y" if (route == 0) == (phase == 1) else "z"
            for sign in (1, -1):
                if k <= hops(s, phase, sign):
                    pieces = slice(None) if (phase, k) != (2, 4) else slice(0, 4) if sign > 0 else slice(4, 8)
                    ref = slab(s, route, phase, near(axis, -sign * (k - 1)), pieces)
                    send(ref, ref, at(axis, sign), ("w", s, phase, k))
        if s in EARLY and phase == 1:
            send_ahead(s, ahead(k))

    def finish(s):
        arrived(("w", s, 2, 4))

    def gather(B, tag):
        lo, hi = slice(0, ROWS // 2), slice(ROWS // 2, ROWS)
        right, left, other = at("x", 1), at("x", -1), at("c", 1)
        from_left, from_right, across = (2 * near("x", o) + c for o in (-1, 1, 2))

        def pass_on(block, half, device, group):
            ref = B.at[block, half]
            send(ref, ref, device, (tag, group))

        def start():
            pass_on(me, lo, right, "near")
            pass_on(me, hi, left, "near")
            pass_on(me, hi, right, "next")
            pass_on(me, lo, left, "next")
            send(B.at[me], B.at[me], other, (tag, "d"))

        def relay():
            arrived((tag, "near"))
            pass_on(from_left, lo, right, "far")
            pass_on(from_right, hi, left, "far")
            pass_on(from_left, lo, other, "d")
            pass_on(from_right, hi, other, "d")

        def rest():
            arrived((tag, "next"))
            pass_on(from_left, hi, other, "d")
            pass_on(from_right, lo, other, "d")

        def far():
            arrived((tag, "far"))
            pass_on(across, lo, other, "d")
            pass_on(across, hi, other, "d")

        def end():
            arrived((tag, "d"))

        return start, relay, rest, far, end

    def scatter(S, Q, U, RL, F, tag):
        n = S.shape[2]
        lo, hi = slice(0, n // 2), slice(n // 2, n)
        right, left, other = at("x", 1), at("x", -1), at("c", 1)

        def hand_over(offset):
            b = near("x", offset)
            send(S.at[b, near("c", 1)], Q.at[b], other, (tag, "q", abs(offset)))

        def pair(offset, half):
            b = near("x", offset)
            return S[b, c, half, :].astype(F32) + Q[b, half, :].astype(F32)

        def first():
            arrived((tag, "q", 2))
            U[2, lo, :] = pair(2, lo).astype(BF16)
            send(U.at[2, lo], RL.at[lo], right, (tag, "far"))
            U[2, hi, :] = pair(2, hi).astype(BF16)
            send(U.at[2, hi], RL.at[hi], left, (tag, "far"))

        def second():
            arrived((tag, "q", 1))
            U[0, hi, :] = pair(1, hi).astype(BF16)
            send(U.at[0, hi], F.at[0, hi], right, (tag, "near"))
            U[1, lo, :] = pair(-1, lo).astype(BF16)
            send(U.at[1, lo], F.at[1, lo], left, (tag, "near"))

        def third():
            arrived((tag, "far"))
            U[0, lo, :] = (pair(1, lo) + RL[lo, :].astype(F32)).astype(BF16)
            send(U.at[0, lo], F.at[0, lo], right, (tag, "near"))
            U[1, hi, :] = (pair(-1, hi) + RL[hi, :].astype(F32)).astype(BF16)
            send(U.at[1, hi], F.at[1, hi], left, (tag, "near"))

        def total():
            arrived((tag, "q", 0))
            arrived((tag, "near"))
            return pair(0, slice(0, n)) + F[0].astype(F32) + F[1].astype(F32)

        return hand_over, first, second, third, total

    def norm(B, gain):
        def rows_of(i, carry):
            rows = pl.ds(pl.multiple_of(i * 128, 128), 128)
            squares = jnp.zeros((128, COLS), F32)
            for j in range(8):
                v = B[j, rows, :].astype(F32)
                squares = squares + v * v
            r = lax.rsqrt(jnp.sum(squares, axis=1, keepdims=True) * (1.0 / D) + EPS)
            for j in range(8):
                lanes = slice(COLS * j, COLS * j + COLS)
                N[rows, lanes] = (B[j, rows, :].astype(F32) * r * gain[:, lanes]).astype(BF16)
            return carry

        lax.fori_loop(0, 3, rows_of, 0)

    gather1, gather2 = gather(T, "g1"), gather(M, "g2")
    scatter1 = scatter(S1, Q1, U1, RL1, F1, "s1")
    scatters = (
        scatter(S2, Q2, U2, RL2, F2, "s2"), scatter(S3, Q3, U3, RL3, F3, "s3"),
    )

    def mixer():
        finish(MIX[0])
        pooled_in = jnp.dot(N[...], PIN[...].reshape(D, 128), preferred_element_type=F32).astype(BF16)
        window = jnp.left_shift(jnp.int32(2), lax.rem(me, 4))
        later = lax.broadcasted_iota(jnp.int32, (LENGTH, LENGTH), 0)
        earlier = lax.broadcasted_iota(jnp.int32, (LENGTH, LENGTH), 1)
        inside = (earlier <= later) & (earlier > later - window)
        band = jnp.where(inside, 1.0, 0.0).astype(BF16)
        divisor = jnp.minimum(later + 1, window).astype(F32)
        grouped = []
        for s in range(ROWS // LENGTH):
            own = pooled_in[s * LENGTH : (s + 1) * LENGTH]
            sums = jnp.dot(band, own, preferred_element_type=F32)
            pooled = (sums / divisor - own.astype(F32)).astype(BF16)
            mapped = jnp.dot(pooled, group_weight[...], preferred_element_type=F32)
            grouped.append((mapped * channel_scale[...]).astype(BF16))
        GR[...] = jnp.concatenate(grouped, axis=0)

    def mixer_first():
        finish(MIX[1])
        mixer_out(2)

    def mixer_out(*offsets):
        for offset in offsets:
            b = near("x", offset)
            for core in (near("c", 1), c):
                piece = POUT[2 * b + core].reshape(COLS, 128)
                terms = lax.dot_general(GR[...], piece, (((1,), (1,)), ((), ())), preferred_element_type=F32)
                S1[b, core] = terms.astype(BF16)
            scatter1[0](offset)

    def middle():
        value = (T[me].astype(F32) + scatter1[4]()).astype(BF16)
        M[me] = value
        gather2[0]()
        MT[...] = jnp.transpose(value.astype(F32)).reshape(8, 32, ROWS)

    def silu_up(g, u):
        return g / (1.0 + jnp.exp(-g)) * u

    settled = set()

    def settle(i):
        for s in tile_streams(i):
            if s not in settled:
                finish(s)
                settled.add(s)

    def hidden(i):
        settle(i)
        piece = GU[:, :, :, 256 * i : 256 * i + 256].reshape(D, 256)
        acc = jnp.dot(N[...], piece, preferred_element_type=F32)
        h = silu_up(acc[:, :128], acc[:, 128:])
        HT[128 * i : 128 * i + 128, :] = jnp.transpose(h).astype(BF16)

    def hidden_tail():
        settle(5)
        acc = jnp.dot(N[...], GU[:, :, :, 1280:1408].reshape(D, 128), preferred_element_type=F32)
        h = silu_up(acc, pltpu.roll(acc, 64, 1))
        lane = lax.broadcasted_iota(jnp.int32, h.shape, 1)
        h = jnp.where(lane < 64, h, 0.0)
        HTT[0] = jnp.transpose(h).astype(BF16)
        HTT[1] = jnp.transpose(pltpu.roll(h, 64, 1)).astype(BF16)

    def down(h, S, offset):
        if offset == 2:
            if h == 0:
                finish(TAIL)
            finish(DOWN[h])
        b = near("x", offset)
        rows = DOWN_ROWS[h][1]
        both = pl.ds(2 * b, 2)
        end = jnp.concatenate([DTA[both], DTB[both]], axis=2).reshape(16 * rows, 128)
        piece = jnp.concatenate([DN[h][both].reshape(16 * rows, 640), end], axis=1)
        right = jnp.concatenate([HT[...], HTT[h]], axis=0)
        terms = jnp.dot(piece, right, preferred_element_type=F32).astype(BF16)
        S[b] = terms.reshape(2, 8 * rows, ROWS)
        scatters[h][0](offset)

    def collect(h):
        first, rows = DOWN_ROWS[h]
        part_of = slice(first, first + rows)
        C[:, part_of] = scatters[h][4]().reshape(8, rows, ROWS) + MT[:, part_of]

    def last():
        closing = C[...].reshape(COLS, ROWS)
        own = jnp.sum(closing * closing, axis=0, keepdims=True)
        SQ[me] = jnp.broadcast_to(own, (8, ROWS))
        for peer in peers:
            send(SQ.at[me], SQ.at[me], peer, "squares")
        arrived("squares")
        squares = jnp.sum(SQ[...], axis=0)[0:1]
        scaled = C[...].reshape(COLS, ROWS) * lax.rsqrt(squares * (1.0 / D) + EPS)
        out[...] = (jnp.transpose(scaled) * final_gain[...]).astype(BF16)

    runs = {"norm1": lambda: norm(T, mixer_gain), "mixer": mixer, "mixer0": mixer_first, "mixer1": lambda: mixer_out(1, -1),
            "mixer2": lambda: mixer_out(0), "middle": middle, "norm2": lambda: norm(M, ffn_gain)}
    for s in range(len(STREAMS)):
        runs["w", s, 0, 4] = lambda s=s: spread(s)
        for phase in (1, 2):
            for k in range(1, 5):
                runs["w", s, phase, k] = lambda s=s, phase=phase, k=k: step(s, phase, k)
    for tag, parts in (("g1", gather1), ("g2", gather2), ("s1", scatter1), ("s2", scatters[0]), ("s3", scatters[1])):
        for i, part_run in enumerate(parts):
            runs[tag, i] = part_run
    runs["g2", 0] = lambda: None
    for i in range(5):
        runs["h", i] = lambda i=i: hidden(i)
    runs["h", 5] = hidden_tail
    for h, S in enumerate((S2, S3)):
        runs["c", h] = lambda h=h: collect(h)
        for offset in (2, 1, -1, 0):
            runs["d", h, offset] = lambda h=h, S=S, offset=offset: down(h, S, offset)
    runs["last"] = last
    for t, name in order(events()):
        next_event()
        runs[name]()
    for slot in range(SENDING):
        drain(slot)


def scatter_scratch(n, lanes):
    return [
        pltpu.VMEM((4, 2, n, lanes), BF16),
        pltpu.VMEM((4, n, lanes), BF16),
        pltpu.VMEM((3, n, lanes), BF16),
        pltpu.VMEM((n, lanes), BF16),
        pltpu.VMEM((2, n, lanes), BF16),
    ]


def local(
    tokens, mixer_gain, pool_input, group_weight, channel_scale, pool_output,
    ffn_gain, gate_weight, up_weight, down_weight, final_gain,
):
    vmem = pl.BlockSpec(memory_space=pltpu.VMEM)
    hbm = pl.BlockSpec(memory_space=pltpu.HBM)
    operands = (
        tokens, pool_input, pool_output.T, gate_weight, up_weight, down_weight.T, mixer_gain.reshape(1, D),
        group_weight.reshape(128, 128), channel_scale.reshape(1, 128), ffn_gain.reshape(1, D), final_gain.reshape(1, COLS),
    )
    return pl.pallas_call(
        kernel,
        out_shape=jax.ShapeDtypeStruct((ROWS, COLS), BF16),
        in_specs=[hbm] * 11,
        out_specs=vmem,
        scratch_shapes=[
            pltpu.VMEM((8, ROWS, COLS), BF16),
            pltpu.VMEM((8, ROWS, COLS), BF16),
            pltpu.VMEM((8, 8, 32, 128), BF16),
            pltpu.VMEM((8, 8, 32, 128), BF16),
            pltpu.VMEM((8, 8, 32, 1408), BF16),
            *(pltpu.VMEM((8, 8, rows, 640), BF16) for _, rows in DOWN_ROWS),
            pltpu.VMEM((8, 8, 8, 128), BF16),
            pltpu.VMEM((8, 8, 8, 128), BF16),
            pltpu.VMEM((ROWS, D), BF16),
            pltpu.VMEM((ROWS, 128), BF16),
            pltpu.VMEM((640, ROWS), BF16),
            pltpu.VMEM((2, 128, ROWS), BF16),
            pltpu.VMEM((8, 32, ROWS), F32),
            pltpu.VMEM((8, 32, ROWS), F32),
            pltpu.VMEM((8, 8, ROWS), F32),
            pltpu.VMEM((32, 704), BF16),
            pltpu.VMEM((32, 704), BF16),
            pltpu.VMEM((32, 704), BF16),
            pltpu.VMEM((1, D), F32),
            pltpu.VMEM((128, 128), BF16),
            pltpu.VMEM((1, 128), F32),
            pltpu.VMEM((1, D), F32),
            pltpu.VMEM((1, COLS), F32),
            *scatter_scratch(ROWS, COLS),
            *(s for _, rows in DOWN_ROWS for s in scatter_scratch(8 * rows, ROWS)),
            pltpu.VMEM((3072, 128), BF16),
            pltpu.SemaphoreType.DMA((11,)),
            pltpu.SemaphoreType.DMA((SENDING,)),
            pltpu.SemaphoreType.DMA((ARRIVALS,)),
        ],
        compiler_params=pltpu.CompilerParams(
            collective_id=0, has_side_effects=True, vmem_limit_bytes=50 * 1024 * 1024
        ),
        name="layer",
    )(*(pltpu.with_memory_space_constraint(a, pltpu.HBM) for a in operands))


def solution(mesh):
    torus = Mesh(mesh.devices.reshape(8, 8, 4, 2), ("z", "y", "x", "c"))
    in_specs = (
        P(FS, TP),
        P(),
        P(FS, TP),
        P(TP, None, None),
        P(TP),
        P(TP, FS),
        P(),
        P(FS, TP),
        P(FS, TP),
        P(TP, FS),
        P(TP),
    )
    return jax.shard_map(local, mesh=torus, in_specs=in_specs, out_specs=P(FS, TP), check_vma=False)
```
